256 devices in a mesh: kv: 32 (over z, y), tp: 8 (over x, core).
Axes of the slice: x: 4, y: 4, z: 8, core: 2. Of those that a mesh axis runs over, the one named last changes fastest.
Arguments:
- tokens: bfloat16 [512, 4096], P('tp', 'kv')
- seq_pos: int32 [512], P('kv'), may hold values from 0 to 4095
- state: float32 [512, 16, 128, 256], P('kv', 'tp'), may hold values from -0.6 to 0.6
- norm_in_gain: float32 [4096], P('kv'), may hold values from 0.1 to 1.9
- query_weight: bfloat16 [4096, 2048], P('kv', 'tp'), may hold values from -0.09375 to 0.09375
- key_weight: bfloat16 [4096, 2048], P('kv', 'tp'), may hold values from -0.09375 to 0.09375
- value_weight: bfloat16 [4096, 4096], P('kv', 'tp'), may hold values from -0.09375 to 0.09375
- gate_weight: bfloat16 [4096, 4096], P('kv', 'tp'), may hold values from -0.09375 to 0.09375
- head_gain: float32 [4096], P('tp'), may hold values from 0.1 to 1.9
- out_weight: bfloat16 [4096, 4096], P('tp', 'kv'), may hold values from -0.09375 to 0.09375
- norm_mlp_gain: float32 [4096], P('kv'), may hold values from 0.1 to 1.9
- hidden_weight: bfloat16 [4096, 16384], P('kv', 'tp'), may hold values from -0.09375 to 0.09375
- down_weight: bfloat16 [16384, 4096], P('tp', 'kv'), may hold values from -0.046875 to 0.046875
Outputs:
- output: bfloat16 [512, 4096], P('tp', 'kv')
- new_state: float32 [512, 16, 128, 256], P('kv', 'tp')
The draws below stay inside these ranges and needn't reach their ends.
All inputs are finite; a program needn't handle non-finite values.
Results may differ from the reference program's by a relative error of at most 0.03.
Values may be sent and summed in bfloat16 or wider, within the bound.
No kernel may reach another device: no remote copies, remote signals or barrier semaphores. Data moves between devices by JAX's collectives and lax.ppermute only.
A program may use at most 64 MiB of HBM per device.

```python
import jax
import jax.numpy as jnp
from jax import lax

D = 4096
H = 16
DK = 128
DV = 256
FF = 16384
BATCH = 512
N_KV = 32
N_TP = 8


def draw_tokens(key, part):
    first, second = jax.random.split(key, 2)
    columns = jnp.exp(jnp.log(4.0) * (jnp.arange(D, dtype=jnp.float32) / D - 0.5))
    base = jax.random.normal(first, (BATCH, D), jnp.float32)
    rows = jnp.exp(jax.random.uniform(second, (BATCH, 1), jnp.float32, jnp.log(0.25), jnp.log(2.5)))
    return (base * rows * columns[None, :]).astype(jnp.bfloat16)


def place_ends(result, rng, low, top_value):
    longest = result.shape.index(max(result.shape))
    spots = []
    for shift in (0, 1):
        where = [jax.random.randint(jax.random.fold_in(rng, axis), (), 0, length) for axis, length in enumerate(result.shape)]
        where[longest] = (where[longest] + shift) % result.shape[longest]
        spots.append(tuple(where))
    return result.at[spots[0]].set(low).at[spots[1]].set(top_value)


def shard_levels(rng, extent, pieces, smallest, largest):
    def one(axis_at, blocks):
        steps = jax.random.uniform(jax.random.fold_in(jax.random.fold_in(rng, 6), axis_at), (blocks,), jnp.float32, smallest / len(pieces), largest / len(pieces))
        return jnp.repeat(jnp.exp(steps), extent[axis_at] // blocks).reshape((-1,) + (1,) * (len(extent) - axis_at - 1))

    gain = one(*pieces[0])
    for cut in pieces[1:]:
        gain = gain * one(*cut)
    return gain


def centred(rng, dims, scale, reach, pieces=(), kind=jnp.bfloat16):
    level = shard_levels(rng, dims, pieces, -0.22, 0.18) if pieces else 1.0
    array = jax.random.normal(rng, dims, jnp.float32) * scale * level
    return jnp.minimum(jnp.maximum(array, -reach), reach).astype(kind)


def setup_inputs(seed: int = 0) -> dict:
    seeds = jax.random.split(jax.random.key(seed), 14)
    tokens = draw_tokens(jax.random.fold_in(seeds[13], 71), 0)
    seq_pos = place_ends(jax.random.randint(seeds[1], (BATCH,), 0, 4096), jax.random.fold_in(seeds[1], 1), 0, 4095).astype(jnp.int32)
    state = centred(seeds[2], (BATCH, H, DK, DV), 0.1, 0.6, ((0, 32), (1, 8)), jnp.float32)
    norm_in_gain = jnp.clip(1.0 + 0.18 * jax.random.normal(seeds[3], (D,), jnp.float32), 0.1, 1.9)
    query_weight = centred(seeds[4], (D, H * DK), D ** -0.5, 0.09375, ((0, 32), (1, 8)))
    key_weight = centred(seeds[5], (D, H * DK), D ** -0.5, 0.09375, ((0, 32), (1, 8)))
    value_weight = centred(seeds[6], (D, H * DV), D ** -0.5, 0.09375, ((0, 32), (1, 8)))
    gate_weight = centred(seeds[7], (D, H * DV), D ** -0.5, 0.09375, ((0, 32), (1, 8)))
    head_gain = jnp.clip(1.0 + 0.18 * jax.random.normal(seeds[8], (H * DV,), jnp.float32), 0.1, 1.9)
    out_weight = centred(seeds[9], (H * DV, D), (H * DV) ** -0.5, 0.09375, ((0, 8), (1, 32)))
    norm_mlp_gain = jnp.clip(1.0 + 0.18 * jax.random.normal(seeds[10], (D,), jnp.float32), 0.1, 1.9)
    hidden_weight = centred(seeds[11], (D, FF), D ** -0.5, 0.09375, ((0, 32), (1, 8)))
    down_weight = centred(seeds[12], (FF, D), FF ** -0.5, 0.046875, ((0, 8), (1, 32)))
    return dict(tokens=tokens, seq_pos=seq_pos, state=state, norm_in_gain=norm_in_gain, query_weight=query_weight, key_weight=key_weight, value_weight=value_weight, gate_weight=gate_weight, head_gain=head_gain, out_weight=out_weight, norm_mlp_gain=norm_mlp_gain, hidden_weight=hidden_weight, down_weight=down_weight)


EPS = 1e-06

def rotate(vectors, positions):
    half = vectors.shape[-1] // 2
    inverse = jnp.power(10000.0, -jnp.arange(half, dtype=jnp.float32) / half)
    angles = positions.astype(jnp.float32)[:, None] * inverse[None, :]
    cosine = jnp.cos(angles)[:, None, :]
    sine = jnp.sin(angles)[:, None, :]
    first, second = (vectors[..., :half], vectors[..., half:])
    return jnp.concatenate([first * cosine - second * sine, first * sine + second * cosine], axis=-1)

def head_decay(head_ids):
    return 1.0 - jnp.exp2(-2.0 - 6.0 * head_ids / (H - 1))

def grouped_sum(left, right, groups):
    width = left.shape[1] // groups
    total = jnp.zeros((left.shape[0], right.shape[1]), jnp.float32)
    for group in range(groups):
        piece = jnp.dot(left[:, group * width:(group + 1) * width], right[group * width:(group + 1) * width], preferred_element_type=jnp.float32).astype(jnp.bfloat16)
        total = total + piece.astype(jnp.float32)
    return total

def reference(tokens, seq_pos, state, norm_in_gain, query_weight, key_weight, value_weight, gate_weight, head_gain, out_weight, norm_mlp_gain, hidden_weight, down_weight):
    batch = tokens.shape[0]
    tokens_f = tokens.astype(jnp.float32)
    scale_in = lax.rsqrt(lax.optimization_barrier(jnp.mean(tokens_f * tokens_f, axis=1)) + EPS)[:, None]
    normed_in = (tokens_f * norm_in_gain[None, :]).astype(jnp.bfloat16)
    query = grouped_sum(normed_in, query_weight, N_KV) * scale_in
    keys = grouped_sum(normed_in, key_weight, N_KV) * scale_in
    values = grouped_sum(normed_in, value_weight, N_KV) * scale_in
    gates = grouped_sum(normed_in, gate_weight, N_KV) * scale_in
    turned_query = rotate(query.reshape(batch, H, DK), seq_pos)
    turned_keys = rotate(keys.reshape(batch, H, DK), seq_pos) * DK ** (-0.5)
    decay = head_decay(jnp.arange(H, dtype=jnp.float32))
    new_state = decay[None, :, None, None] * state + jnp.einsum('bhk,bhv->bhkv', turned_keys, values.reshape(batch, H, DV), precision=lax.Precision.HIGHEST)
    read = jnp.einsum('bhk,bhkv->bhv', turned_query, new_state, precision=lax.Precision.HIGHEST)
    read = read * lax.rsqrt(lax.optimization_barrier(jnp.mean(read * read, axis=-1, keepdims=True)) + EPS)
    mixed = (read.reshape(batch, H * DV) * head_gain[None, :] * jax.nn.silu(gates)).astype(jnp.bfloat16)
    attn = grouped_sum(mixed, out_weight, N_TP)
    resid = (tokens_f + attn).astype(jnp.bfloat16)
    resid_f = resid.astype(jnp.float32)
    scale_mid = lax.rsqrt(lax.optimization_barrier(jnp.mean(resid_f * resid_f, axis=1)) + EPS)[:, None]
    normed_mid = (resid_f * norm_mlp_gain[None, :]).astype(jnp.bfloat16)
    hidden = grouped_sum(normed_mid, hidden_weight, N_KV) * scale_mid
    active = jnp.square(jax.nn.relu(hidden)).astype(jnp.bfloat16)
    down = grouped_sum(active, down_weight, N_TP)
    output = (resid_f + down).astype(jnp.bfloat16)
    return (output, new_state)
```

```python
import jax
import jax.numpy as jnp
from jax import lax
from jax.sharding import Mesh
from jax.sharding import PartitionSpec as P

D = 4096
H = 16
DK = 128
DV = 256
KV = ("kv_0", "kv_1")


EPS = 1e-06


def copy_for_each(array, axis):
    copies = jnp.broadcast_to(array, (lax.axis_size(axis), *array.shape))
    return lax.all_to_all(copies, axis, split_axis=0, concat_axis=0, tiled=True)


def in_order(blocks, dim):
    blocks = jnp.moveaxis(blocks, 0, dim)
    shape = blocks.shape
    return blocks.reshape(*shape[:dim], shape[dim] * shape[dim + 1], *shape[dim + 2 :])


def gather_directly(array, axis, dim):
    blocks = copy_for_each(array, axis)
    return in_order(blocks, dim)


def in_blocks(array, dim, devices):
    before, after = (array.shape[:dim], array.shape[dim + 1 :])
    return jnp.moveaxis(array.reshape(*before, devices, -1, *after), dim, 0)


def summed_on_arrival(array, axis, dim):
    devices = lax.axis_size(axis)
    blocks = lax.all_to_all(in_blocks(array, dim, devices), axis, 0, 0, tiled=True)
    return jnp.sum(blocks.astype(jnp.float32), axis=0)


def taken_together(array, axis):
    return copy_for_each(array, axis).sum(axis=0)


def rotate(vectors, positions):
    half = vectors.shape[-1] // 2
    inverse = jnp.power(10000.0, -jnp.arange(half, dtype=jnp.float32) / half)
    angles = positions.astype(jnp.float32)[:, None] * inverse[None, :]
    cosine = jnp.cos(angles)[:, None, :]
    sine = jnp.sin(angles)[:, None, :]
    first, second = (vectors[..., :half], vectors[..., half:])
    return jnp.concatenate(
        [first * cosine - second * sine, first * sine + second * cosine], axis=-1
    )


def head_decay(head_ids):
    return 1.0 - jnp.exp2(-2.0 - 6.0 * head_ids / (H - 1))


def local(
    tokens,
    seq_pos,
    state,
    norm_in_gain,
    query_weight,
    key_weight,
    value_weight,
    gate_weight,
    head_gain,
    out_weight,
    norm_mlp_gain,
    hidden_weight,
    down_weight,
):
    rows_all = gather_directly(tokens, "tp", 0)
    rows_f = rows_all.astype(jnp.float32)
    squares_in = jnp.sum(rows_f * rows_f, axis=1)
    normed_in = (rows_f * norm_in_gain[None, :]).astype(jnp.bfloat16)
    term_query = jnp.dot(normed_in, query_weight, preferred_element_type=jnp.float32).astype(
        jnp.bfloat16
    )
    term_keys = jnp.dot(normed_in, key_weight, preferred_element_type=jnp.float32).astype(
        jnp.bfloat16
    )
    term_values = jnp.dot(normed_in, value_weight, preferred_element_type=jnp.float32).astype(
        jnp.bfloat16
    )
    term_gates = jnp.dot(normed_in, gate_weight, preferred_element_type=jnp.float32).astype(
        jnp.bfloat16
    )
    terms = jnp.concatenate(
        [term_query, term_keys, term_values, term_gates, squares_in.astype(jnp.bfloat16)[:, None]],
        axis=1,
    )
    sums = summed_on_arrival(terms, KV, 0)
    wq, wv = (query_weight.shape[1], value_weight.shape[1])
    query, keys = (sums[:, :wq], sums[:, wq : 2 * wq])
    values, gates = (sums[:, 2 * wq : 2 * wq + wv], sums[:, 2 * wq + wv : 2 * wq + 2 * wv])
    total_in = sums[:, -1]
    factor = lax.rsqrt(total_in / D + EPS)[:, None]
    query, keys, values, gates = (query * factor, keys * factor, values * factor, gates * factor)
    local_rows = query.shape[0]
    heads_dev = H // lax.axis_size("tp")
    turned_query = rotate(query.reshape(local_rows, heads_dev, DK), seq_pos)
    turned_keys = rotate(keys.reshape(local_rows, heads_dev, DK), seq_pos) * DK ** (-0.5)
    head_ids = (lax.axis_index("tp") * heads_dev + jnp.arange(heads_dev, dtype=jnp.int32)).astype(
        jnp.float32
    )
    decay = head_decay(head_ids)
    new_state = decay[None, :, None, None] * state + jnp.einsum(
        "bhk,bhv->bhkv",
        turned_keys,
        values.reshape(local_rows, heads_dev, DV),
        precision=lax.Precision.HIGHEST,
    )
    read = jnp.einsum("bhk,bhkv->bhv", turned_query, new_state, precision=lax.Precision.HIGHEST)
    read = read * lax.rsqrt(jnp.mean(read * read, axis=-1, keepdims=True) + EPS)
    mixed = (
        read.reshape(local_rows, heads_dev * DV) * head_gain[None, :] * jax.nn.silu(gates)
    ).astype(jnp.bfloat16)
    attn_terms = jnp.dot(
        gather_directly(mixed, KV, 0), out_weight, preferred_element_type=jnp.float32
    )
    attn = summed_on_arrival(attn_terms.astype(jnp.bfloat16), "tp", 0)
    resid = (tokens.astype(jnp.float32) + attn).astype(jnp.bfloat16)
    resid_all = gather_directly(resid, "tp", 0)
    resid_f = resid_all.astype(jnp.float32)
    squares_mid = jnp.sum(resid_f * resid_f, axis=1)
    normed_mid = (resid_f * norm_mlp_gain[None, :]).astype(jnp.bfloat16)
    term_hidden = jnp.dot(normed_mid, hidden_weight, preferred_element_type=jnp.float32).astype(
        jnp.bfloat16
    )
    total_mid = taken_together(squares_mid, KV)
    scale_mid = lax.rsqrt(total_mid / D + EPS)[:, None]
    hidden = summed_on_arrival(term_hidden, KV, 0)
    row_start = lax.axis_index(KV) * hidden.shape[0]
    local_scale = lax.dynamic_slice_in_dim(scale_mid, row_start, hidden.shape[0], 0)
    active = jnp.square(jax.nn.relu(hidden * local_scale)).astype(jnp.bfloat16)
    down_terms = jnp.dot(
        gather_directly(active, KV, 0), down_weight, preferred_element_type=jnp.float32
    )
    down = summed_on_arrival(down_terms.astype(jnp.bfloat16), "tp", 0)
    output = (resid.astype(jnp.float32) + down).astype(jnp.bfloat16)
    return (output, new_state)


def solution(mesh):
    torus = Mesh(mesh.devices.reshape(8, 4, mesh.shape["tp"]), ("kv_0", "kv_1", "tp"))
    return jax.shard_map(
        local,
        mesh=torus,
        in_specs=(
            P("tp", KV),
            P(KV),
            P(KV, "tp", None, None),
            P(KV),
            P(KV, "tp"),
            P(KV, "tp"),
            P(KV, "tp"),
            P(KV, "tp"),
            P("tp"),
            P("tp", KV),
            P(KV),
            P(KV, "tp"),
            P("tp", KV),
        ),
        out_specs=(P("tp", KV), P(KV, "tp", None, None)),
        check_vma=False,
    )
```

```python
import jax
import jax.numpy as jnp
from jax import lax
from jax.experimental import pallas as pl
from jax.sharding import Mesh
from jax.sharding import PartitionSpec as P

D = 4096
H = 16
DK = 128
DV = 256
KV = ("z", "y")
TP = ("x", "c")
ZX = ("z", "x")
NZ, NY, NX, NC = (8, 4, 4, 2)


EPS = 1e-06


def exchanged(blocks, axis):
    return lax.all_to_all(blocks, axis, split_axis=0, concat_axis=0, tiled=True)


def copy_for_each(array, axis):
    copies = jnp.broadcast_to(array, (lax.axis_size(axis), *array.shape))
    return exchanged(copies, axis)


def summed_on_arrival(blocks, axis):
    return jnp.sum(exchanged(blocks, axis).astype(jnp.float32), axis=0)


def shifted(array, axis, by):
    size = lax.axis_size(axis)
    return lax.ppermute(array, axis, [(i, (i + by) % size) for i in range(size)])


def swapped(array):
    return lax.ppermute(array, "c", [(0, 1), (1, 0)])


def rotate(vectors, positions):
    half = vectors.shape[-1] // 2
    inverse = jnp.power(10000.0, -jnp.arange(half, dtype=jnp.float32) / half)
    angles = positions.astype(jnp.float32)[:, None] * inverse[None, :]
    cosine = jnp.cos(angles)[:, None, :]
    sine = jnp.sin(angles)[:, None, :]
    first, second = (vectors[..., :half], vectors[..., half:])
    return jnp.concatenate(
        [first * cosine - second * sine, first * sine + second * cosine], axis=-1
    )


def head_decay(head_ids):
    return 1.0 - jnp.exp2(-2.0 - 6.0 * head_ids / (H - 1))


def mixer_kernel(own_ref, other_ref, w0_ref, w1_ref, w2a_ref, w2b_ref, w3_ref, out_own_ref, out_other_ref):
    rows = own_ref.shape[1]
    half = NZ // 2

    def weights(z, low, high):
        far = w2a_ref[z, low:high] if z < half else w2b_ref[z - half, low:high]
        return [w0_ref[z, low:high], w1_ref[z, low:high], far, w3_ref[z, low:high]]

    hidden = jnp.zeros((2 * rows, 256), jnp.float32)
    squares = jnp.zeros((2 * rows, 1), jnp.float32)
    for z in range(NZ):
        left = jnp.concatenate([own_ref[z], other_ref[z]], axis=0)
        wide = left.astype(jnp.float32)
        squares = squares + jnp.sum(wide * wide, axis=1, keepdims=True)
        right = [jnp.concatenate(weights(z, 128 * j, 128 * (j + 1)), axis=0) for j in range(2)]
        right = jnp.concatenate(right, axis=1)
        hidden = hidden + jnp.dot(left, right, preferred_element_type=jnp.float32)
    scale = lax.rsqrt(squares / D + EPS)
    positive = jnp.maximum(hidden * scale, 0.0)
    active = (positive * positive).astype(jnp.bfloat16)
    for z in range(NZ):
        right = jnp.concatenate(weights(z, 256, 512), axis=1)
        out = jnp.dot(active, right, preferred_element_type=jnp.float32)
        out_own_ref[z] = out[:rows].astype(jnp.bfloat16)
        out_other_ref[z] = out[rows:].astype(jnp.bfloat16)


def ring(array):
    above = shifted(array, "y", -1)
    below = shifted(array, "y", 1)
    return above, below


def local(
    tokens,
    seq_pos,
    state,
    norm_in_gain,
    query_weight,
    key_weight,
    value_weight,
    gate_weight,
    head_gain,
    out_weight,
    norm_mlp_gain,
    hidden_weight,
    down_weight,
):
    y = lax.axis_index("y")
    weights = jnp.concatenate([query_weight, key_weight, value_weight, gate_weight], axis=1)
    weights = (weights.astype(jnp.float32) * norm_in_gain[:, None]).astype(jnp.bfloat16)
    width = weights.shape[1]
    above, below = ring(weights)
    far_a = shifted(below[:, : width // 2], "y", 1)
    far_b = shifted(above[:, width // 2 :], "y", -1)

    rows = jnp.broadcast_to(tokens.reshape(NY, 1, 16, 128), (NY, NX * NC, 16, 128))
    rows = exchanged(rows.reshape(NY * NX * NC, 16, 128), ("y", "x", "c"))
    rows = rows.reshape(NY, 128, 128)
    rows = lax.dynamic_slice_in_dim(jnp.concatenate([rows, rows], axis=0), y, NY, 0)

    scaled = (hidden_weight.astype(jnp.float32) * norm_mlp_gain[:, None]).astype(jnp.bfloat16)
    scaled = scaled.reshape(128, NZ, 2, 128).transpose(1, 2, 0, 3).reshape(NZ, 256, 128)
    mixer = jnp.concatenate([scaled, down_weight.reshape(NZ, 256, 128)], axis=1)
    mixer = exchanged(mixer, "z")

    def term(left, right):
        return jnp.dot(left, right, preferred_element_type=jnp.float32)

    near = term(rows[0], weights) + term(rows[3], below) + term(rows[1], above)
    far = jnp.concatenate([term(rows[2], far_a), term(rows[2], far_b)], axis=1)
    rows_f = rows.astype(jnp.float32)
    squares = jnp.sum(rows_f * rows_f, axis=(0, 2))[:, None]
    coarse = squares.astype(jnp.bfloat16)
    fine = (squares - coarse.astype(jnp.float32)).astype(jnp.bfloat16)
    terms = jnp.concatenate([(near + far).astype(jnp.bfloat16), coarse, fine], axis=1)
    sums = summed_on_arrival(terms.reshape(NZ, 16, width + 2), "z")
    total_in = sums[:, width] + sums[:, width + 1]
    factor = lax.rsqrt(total_in / D + EPS)[:, None]
    wq, wv = (query_weight.shape[1], value_weight.shape[1])
    query = sums[:, :wq] * factor
    keys = sums[:, wq : 2 * wq] * factor
    values = sums[:, 2 * wq : 2 * wq + wv] * factor
    gates = sums[:, 2 * wq + wv : width] * factor

    mix_above, mix_below = ring(mixer)
    out_above, out_below = ring(out_weight)
    out_far = shifted(out_weight, "y", 2)
    out_wide = jnp.concatenate([out_weight, out_above, out_far, out_below], axis=1)

    local_rows = query.shape[0]
    heads_dev = 2
    turned_query = rotate(query.reshape(local_rows, heads_dev, DK), seq_pos)
    turned_keys = rotate(keys.reshape(local_rows, heads_dev, DK), seq_pos) * DK ** (-0.5)
    head_ids = (lax.axis_index(TP) * heads_dev + jnp.arange(heads_dev, dtype=jnp.int32)).astype(
        jnp.float32
    )
    decay = head_decay(head_ids)
    new_state = decay[None, :, None, None] * state + jnp.einsum(
        "bhk,bhv->bhkv",
        turned_keys,
        values.reshape(local_rows, heads_dev, DV),
        precision=lax.Precision.HIGHEST,
    )
    read = jnp.einsum("bhk,bhkv->bhv", turned_query, new_state, precision=lax.Precision.HIGHEST)
    read = read * lax.rsqrt(jnp.mean(read * read, axis=-1, keepdims=True) + EPS)
    mixed = (
        read.reshape(local_rows, heads_dev * DV) * head_gain[None, :] * jax.nn.silu(gates)
    ).astype(jnp.bfloat16)
    mixed_all = copy_for_each(mixed, "z").reshape(128, heads_dev * DV)
    attn_terms = term(mixed_all, out_wide).astype(jnp.bfloat16)
    attn = summed_on_arrival(attn_terms.reshape(NX * NC, 16, 512), TP)
    mine = rows.reshape(NY, NX * NC, 16, 128)
    mine = lax.dynamic_index_in_dim(mine, lax.axis_index(TP), 1, keepdims=False)
    mine = mine.transpose(1, 0, 2).reshape(16, 512)
    resid = (mine.astype(jnp.float32) + attn).astype(jnp.bfloat16)

    far_low = shifted(mix_below[: NZ // 2], "y", 1)
    far_high = shifted(mix_above[NZ // 2 :], "y", -1)

    own = copy_for_each(resid, ZX).reshape(NZ, 64, 512)
    other = swapped(own)
    blocks = jax.ShapeDtypeStruct((NZ, 64, 512), jnp.bfloat16)
    out_own, out_other = pl.pallas_call(
        mixer_kernel,
        out_shape=(blocks, blocks),
        name="mixer",
    )(own, other, mixer, mix_above, far_low, far_high, mix_below)
    from_other = swapped(out_other)
    partial = (out_own.astype(jnp.float32) + from_other.astype(jnp.float32)).astype(jnp.bfloat16)
    down = summed_on_arrival(partial.reshape(NZ * NX, 16, 512), ZX)
    output = (resid.astype(jnp.float32) + down).astype(jnp.bfloat16)
    output = output.reshape(16, NY, 128).transpose(1, 0, 2)
    output = jnp.concatenate([output, output], axis=0)
    output = lax.dynamic_slice_in_dim(output, (NY - y) % NY, NY, 0)
    output = exchanged(output, "y").reshape(64, 128)
    return (output, new_state)


def solution(mesh):
    torus = Mesh(mesh.devices.reshape(NZ, NY, NX, NC), ("z", "y", "x", "c"))
    return jax.shard_map(
        local,
        mesh=torus,
        in_specs=(
            P(TP, KV),
            P(KV),
            P(KV, TP, None, None),
            P(KV),
            P(KV, TP),
            P(KV, TP),
            P(KV, TP),
            P(KV, TP),
            P(TP),
            P(TP, KV),
            P(KV),
            P(KV, TP),
            P(TP, KV),
        ),
        out_specs=(P(TP, KV), P(KV, TP, None, None)),
        check_vma=False,
    )
```

```python
import jax
import jax.numpy as jnp
from jax import lax
from jax.experimental import pallas as pl
from jax.experimental.pallas import tpu as pltpu
from jax.sharding import Mesh
from jax.sharding import PartitionSpec as P

D = 4096
H = 16
DK = 128
DV = 256
KV = ("z", "y")
TP = ("x", "c")
ZX = ("z", "x")
NZ, NY, NX, NC = (8, 4, 4, 2)


EPS = 1e-06


def exchanged(blocks, axis):
    return lax.all_to_all(blocks, axis, split_axis=0, concat_axis=0, tiled=True)


def copy_for_each(array, axis):
    copies = jnp.broadcast_to(array, (lax.axis_size(axis), *array.shape))
    return exchanged(copies, axis)


def summed_on_arrival(blocks, axis):
    return jnp.sum(exchanged(blocks, axis).astype(jnp.float32), axis=0)


def shifted(array, axis, by):
    size = lax.axis_size(axis)
    return lax.ppermute(array, axis, [(i, (i + by) % size) for i in range(size)])


def swapped(array):
    return lax.ppermute(array, "c", [(0, 1), (1, 0)])


def rotate(vectors, positions):
    half = vectors.shape[-1] // 2
    inverse = jnp.power(10000.0, -jnp.arange(half, dtype=jnp.float32) / half)
    angles = positions.astype(jnp.float32)[:, None] * inverse[None, :]
    cosine = jnp.cos(angles)[:, None, :]
    sine = jnp.sin(angles)[:, None, :]
    first, second = (vectors[..., :half], vectors[..., half:])
    return jnp.concatenate(
        [first * cosine - second * sine, first * sine + second * cosine], axis=-1
    )


def head_decay(head_ids):
    return 1.0 - jnp.exp2(-2.0 - 6.0 * head_ids / (H - 1))


def far_block(low_ref, high_ref, z, size):
    half = NZ // 2
    ref, at = (low_ref, z) if z < half else (high_ref, z - half)
    return ref.at[pl.ds(at * size, size)]


def hidden_kernel(own_ref, other_ref, w0_ref, w1_ref, w2a_ref, w2b_ref, w3_ref, out_ref, x_ref, w_ref, x_sem, w_sem):
    me = lax.axis_index("c")
    copies = []
    for z in range(NZ):
        parts = [
            pltpu.make_async_copy(own_ref.at[z], x_ref.at[z, me], x_sem.at[z, 0]),
            pltpu.make_async_copy(other_ref.at[z], x_ref.at[z, 1 - me], x_sem.at[z, 1]),
        ]
        far = w2a_ref.at[z] if z < NZ // 2 else w2b_ref.at[z - NZ // 2]
        for r, ref in enumerate([w0_ref.at[z], w1_ref.at[z], far, w3_ref.at[z]]):
            parts.append(pltpu.make_async_copy(ref, w_ref.at[z, r], w_sem.at[z, r]))
        for copy in parts:
            copy.start()
        copies.append(parts)
    rows = own_ref.shape[1]
    hidden = jnp.zeros((2 * rows, 256), jnp.float32)
    squares = jnp.zeros((2 * rows, 1), jnp.float32)
    for z in range(NZ):
        for copy in copies[z]:
            copy.wait()
        left = x_ref[z].reshape(2 * rows, 512)
        wide = left.astype(jnp.float32)
        squares = squares + jnp.sum(wide * wide, axis=1, keepdims=True)
        right = [w_ref[z, :, 128 * j : 128 * (j + 1), :].reshape(512, 128) for j in range(2)]
        right = jnp.concatenate(right, axis=1)
        hidden = hidden + jnp.dot(left, right, preferred_element_type=jnp.float32)
    scale = lax.rsqrt(squares / D + EPS)
    positive = jnp.maximum(hidden * scale, 0.0)
    active = (positive * positive).astype(jnp.bfloat16)
    for z in range(NZ):
        out_ref[z] = active


def down_kernel(act_ref, resid_ref, w0_ref, w1_ref, w2a_ref, w2b_ref, w3_ref, out_ref, a_ref, w_ref, a_sem, w_sem):
    y, x, c = (lax.axis_index("y"), lax.axis_index("x"), lax.axis_index("c"))
    copies = []
    for z in range(NZ):
        parts = [pltpu.make_async_copy(act_ref.at[z], a_ref.at[z], a_sem.at[z])]
        near = [ref.at[pl.ds(256 * z, 256)] for ref in (w0_ref, w1_ref, w3_ref)]
        blocks = [near[0], near[1], far_block(w2a_ref, w2b_ref, z, 256), near[2]]
        for r, ref in enumerate(blocks):
            parts.append(pltpu.make_async_copy(ref, w_ref.at[z, r], w_sem.at[z, r]))
        for copy in parts:
            copy.start()
        copies.append(parts)
    total = jnp.zeros((128, 512), jnp.float32)
    for z in range(NZ):
        for copy in copies[z]:
            copy.wait()
        right = jnp.concatenate([w_ref[z, r] for r in range(NY)], axis=1)
        total = total + jnp.dot(a_ref[z], right, preferred_element_type=jnp.float32)
    resid = resid_ref[...].astype(jnp.float32)
    for cc in range(NC):
        for xx in range(NX):
            rows = total[(cc * NX + xx) * 16 : (cc * NX + xx + 1) * 16]
            mine = jnp.logical_and(x == xx, c == cc)
            rows = (rows + jnp.where(mine, resid, 0.0)).astype(jnp.bfloat16)
            for r in range(NY):
                out_ref[lax.rem(y + r, NY), xx * NC + cc] = rows[:, 128 * r : 128 * (r + 1)]


def ring(array):
    above = shifted(array, "y", -1)
    below = shifted(array, "y", 1)
    return above, below


def local(
    tokens,
    seq_pos,
    state,
    norm_in_gain,
    query_weight,
    key_weight,
    value_weight,
    gate_weight,
    head_gain,
    out_weight,
    norm_mlp_gain,
    hidden_weight,
    down_weight,
):
    y = lax.axis_index("y")
    weights = jnp.concatenate([query_weight, key_weight, value_weight, gate_weight], axis=1)
    weights = (weights.astype(jnp.float32) * norm_in_gain[:, None]).astype(jnp.bfloat16)
    width = weights.shape[1]
    above, below = ring(weights)
    far_a = shifted(below[:, : width // 2], "y", 1)
    far_b = shifted(above[:, width // 2 :], "y", -1)

    rows = jnp.broadcast_to(tokens.reshape(NY, 1, 16, 128), (NY, NX * NC, 16, 128))
    rows = exchanged(rows.reshape(NY * NX * NC, 16, 128), ("y", "x", "c"))
    rows = rows.reshape(NY, 128, 128)
    rows = lax.dynamic_slice_in_dim(jnp.concatenate([rows, rows], axis=0), y, NY, 0)

    scaled = (hidden_weight.astype(jnp.float32) * norm_mlp_gain[:, None]).astype(jnp.bfloat16)
    scaled = scaled.reshape(128, NZ, 2, 128).transpose(1, 2, 0, 3).reshape(NZ, 256, 128)
    mixer = exchanged(scaled, "z")

    def term(left, right):
        return jnp.dot(left, right, preferred_element_type=jnp.float32)

    near = term(rows[0], weights) + term(rows[3], below) + term(rows[1], above)
    far = jnp.concatenate([term(rows[2], far_a), term(rows[2], far_b)], axis=1)
    rows_f = rows.astype(jnp.float32)
    squares = jnp.sum(rows_f * rows_f, axis=(0, 2))[:, None]
    coarse = squares.astype(jnp.bfloat16)
    fine = (squares - coarse.astype(jnp.float32)).astype(jnp.bfloat16)
    terms = jnp.concatenate([(near + far).astype(jnp.bfloat16), coarse, fine], axis=1)
    sums = summed_on_arrival(terms.reshape(NZ, 16, width + 2), "z")
    total_in = sums[:, width] + sums[:, width + 1]
    factor = lax.rsqrt(total_in / D + EPS)[:, None]
    wq, wv = (query_weight.shape[1], value_weight.shape[1])
    query = sums[:, :wq] * factor
    keys = sums[:, wq : 2 * wq] * factor
    values = sums[:, 2 * wq : 2 * wq + wv] * factor
    gates = sums[:, 2 * wq + wv : width] * factor

    mix_above, mix_below = ring(mixer)
    down_above, down_below = ring(down_weight)
    out_above, out_below = ring(out_weight)
    out_far = shifted(out_weight, "y", 2)
    out_wide = jnp.concatenate([out_weight, out_above, out_far, out_below], axis=1)
    out_wide = lax.optimization_barrier(out_wide)

    local_rows = query.shape[0]
    heads_dev = 2
    turned_query = rotate(query.reshape(local_rows, heads_dev, DK), seq_pos)
    turned_keys = rotate(keys.reshape(local_rows, heads_dev, DK), seq_pos) * DK ** (-0.5)
    head_ids = (lax.axis_index(TP) * heads_dev + jnp.arange(heads_dev, dtype=jnp.int32)).astype(
        jnp.float32
    )
    decay = head_decay(head_ids)
    new_state = decay[None, :, None, None] * state + jnp.einsum(
        "bhk,bhv->bhkv",
        turned_keys,
        values.reshape(local_rows, heads_dev, DV),
        precision=lax.Precision.HIGHEST,
    )
    read = jnp.einsum("bhk,bhkv->bhv", turned_query, new_state, precision=lax.Precision.HIGHEST)
    read = read * lax.rsqrt(jnp.mean(read * read, axis=-1, keepdims=True) + EPS)
    mixed = (
        read.reshape(local_rows, heads_dev * DV) * head_gain[None, :] * jax.nn.silu(gates)
    ).astype(jnp.bfloat16)
    mixed_all = copy_for_each(mixed, "z").reshape(128, heads_dev * DV)
    attn_terms = term(mixed_all, out_wide).astype(jnp.bfloat16)
    attn = summed_on_arrival(attn_terms.reshape(NX * NC, 16, 512), TP)
    mine = rows.reshape(NY, NX * NC, 16, 128)
    mine = lax.dynamic_index_in_dim(mine, lax.axis_index(TP), 1, keepdims=False)
    mine = mine.transpose(1, 0, 2).reshape(16, 512)
    resid = (mine.astype(jnp.float32) + attn).astype(jnp.bfloat16)

    far_low = shifted(mix_below[: NZ // 2], "y", 1)
    far_high = shifted(mix_above[NZ // 2 :], "y", -1)

    down_low = shifted(down_below[:1024], "y", 1)
    down_high = shifted(down_above[1024:], "y", -1)

    own = copy_for_each(resid, ZX).reshape(NZ, 64, 512)
    other = swapped(own)
    anywhere = pl.BlockSpec(memory_space=pl.ANY)
    active = pl.pallas_call(
        hidden_kernel,
        out_shape=jax.ShapeDtypeStruct((NZ, 128, 256), jnp.bfloat16),
        in_specs=[anywhere] * 7,
        scratch_shapes=[
            pltpu.VMEM((NZ, NC, 64, 512), jnp.bfloat16),
            pltpu.VMEM((NZ, NY, 256, 128), jnp.bfloat16),
            pltpu.SemaphoreType.DMA((NZ, 2)),
            pltpu.SemaphoreType.DMA((NZ, NY)),
        ],
        name="hidden",
    )(own, other, mixer, mix_above, far_low, far_high, mix_below)
    active = exchanged(active, "z")
    partial = pl.pallas_call(
        down_kernel,
        out_shape=jax.ShapeDtypeStruct((NY, NX * NC, 16, 128), jnp.bfloat16),
        in_specs=[anywhere, pl.BlockSpec(memory_space=pltpu.VMEM)] + [anywhere] * 5,
        scratch_shapes=[
            pltpu.VMEM((NZ, 128, 256), jnp.bfloat16),
            pltpu.VMEM((NZ, NY, 256, 128), jnp.bfloat16),
            pltpu.SemaphoreType.DMA((NZ,)),
            pltpu.SemaphoreType.DMA((NZ, NY)),
        ],
        name="down",
    )(active, resid, down_weight, down_above, down_low, down_high, down_below)
    partial = exchanged(partial.reshape(NY * NX * NC, 16, 128), ("y", "x", "c"))
    output = jnp.sum(partial.reshape(NY, NX * NC, 16, 128).astype(jnp.float32), axis=1)
    output = output.astype(jnp.bfloat16).reshape(64, 128)
    return (output, new_state)


def solution(mesh):
    torus = Mesh(mesh.devices.reshape(NZ, NY, NX, NC), ("z", "y", "x", "c"))
    return jax.shard_map(
        local,
        mesh=torus,
        in_specs=(
            P(TP, KV),
            P(KV),
            P(KV, TP, None, None),
            P(KV),
            P(KV, TP),
            P(KV, TP),
            P(KV, TP),
            P(KV, TP),
            P(TP),
            P(TP, KV),
            P(KV),
            P(KV, TP),
            P(TP, KV),
        ),
        out_specs=(P(TP, KV), P(KV, TP, None, None)),
        check_vma=False,
    )
```

```python
import jax
import jax.numpy as jnp
from jax import lax
from jax.experimental import pallas as pl
from jax.experimental.pallas import tpu as pltpu
from jax.sharding import Mesh
from jax.sharding import PartitionSpec as P

D = 4096
H = 16
DK = 128
DV = 256
KV = ("z", "y")
TP = ("x", "c")
ZX = ("z", "x")
NZ, NY, NX, NC = (8, 4, 4, 2)


EPS = 1e-06


def exchanged(blocks, axis):
    return lax.all_to_all(blocks, axis, split_axis=0, concat_axis=0, tiled=True)


def copy_for_each(array, axis):
    copies = jnp.broadcast_to(array, (lax.axis_size(axis), *array.shape))
    return exchanged(copies, axis)


def summed_on_arrival(blocks, axis):
    return jnp.sum(exchanged(blocks, axis).astype(jnp.float32), axis=0)


def shifted(array, axis, by):
    size = lax.axis_size(axis)
    return lax.ppermute(array, axis, [(i, (i + by) % size) for i in range(size)])


def swapped(array):
    return lax.ppermute(array, "c", [(0, 1), (1, 0)])


def rotate(vectors, positions):
    half = vectors.shape[-1] // 2
    inverse = jnp.power(10000.0, -jnp.arange(half, dtype=jnp.float32) / half)
    angles = positions.astype(jnp.float32)[:, None] * inverse[None, :]
    cosine = jnp.cos(angles)[:, None, :]
    sine = jnp.sin(angles)[:, None, :]
    first, second = (vectors[..., :half], vectors[..., half:])
    return jnp.concatenate(
        [first * cosine - second * sine, first * sine + second * cosine], axis=-1
    )


def head_decay(head_ids):
    return 1.0 - jnp.exp2(-2.0 - 6.0 * head_ids / (H - 1))


def far_block(low_ref, high_ref, z, size):
    half = NZ // 2
    ref, at = (low_ref, z) if z < half else (high_ref, z - half)
    return ref.at[pl.ds(at * size, size)]


def hidden_kernel(own_ref, other_ref, w0_ref, w1_ref, w2a_ref, w2b_ref, w3_ref, out_ref, x_ref, w_ref, x_sem, w_sem):
    me, my_z = (lax.axis_index("c"), lax.axis_index("z"))
    copies = []
    for z in range(NZ):
        at = lax.rem(my_z + NZ - z, NZ)
        parts = [
            pltpu.make_async_copy(own_ref.at[at], x_ref.at[z, me], x_sem.at[z, 0]),
            pltpu.make_async_copy(other_ref.at[at], x_ref.at[z, 1 - me], x_sem.at[z, 1]),
        ]
        far = w2a_ref.at[z] if z < NZ // 2 else w2b_ref.at[z - NZ // 2]
        for r, ref in enumerate([w0_ref.at[z], w1_ref.at[z], far, w3_ref.at[z]]):
            parts.append(pltpu.make_async_copy(ref, w_ref.at[z, r], w_sem.at[z, r]))
        for copy in parts:
            copy.start()
        copies.append(parts)
    rows = own_ref.shape[1]
    hidden = jnp.zeros((2 * rows, 256), jnp.float32)
    squares = jnp.zeros((2 * rows, 1), jnp.float32)
    for z in range(NZ):
        for copy in copies[z]:
            copy.wait()
        left = x_ref[z].reshape(2 * rows, 512)
        wide = left.astype(jnp.float32)
        squares = squares + jnp.sum(wide * wide, axis=1, keepdims=True)
        right = [w_ref[z, :, 128 * j : 128 * (j + 1), :].reshape(512, 128) for j in range(2)]
        right = jnp.concatenate(right, axis=1)
        hidden = hidden + jnp.dot(left, right, preferred_element_type=jnp.float32)
    scale = lax.rsqrt(squares / D + EPS)
    positive = jnp.maximum(hidden * scale, 0.0)
    active = (positive * positive).astype(jnp.bfloat16)
    for z in range(NZ):
        out_ref[z] = active


def down_kernel(act_ref, resid_ref, w0_ref, w1_ref, w2a_ref, w2b_ref, w3_ref, out_ref, a_ref, w_ref, a_sem, w_sem):
    y, x, c = (lax.axis_index("y"), lax.axis_index("x"), lax.axis_index("c"))
    copies = []
    for z in range(NZ):
        parts = [pltpu.make_async_copy(act_ref.at[z], a_ref.at[z], a_sem.at[z])]
        near = [ref.at[pl.ds(256 * z, 256)] for ref in (w0_ref, w1_ref, w3_ref)]
        blocks = [near[0], near[1], far_block(w2a_ref, w2b_ref, z, 256), near[2]]
        for r, ref in enumerate(blocks):
            parts.append(pltpu.make_async_copy(ref, w_ref.at[z, r], w_sem.at[z, r]))
        for copy in parts:
            copy.start()
        copies.append(parts)
    total = jnp.zeros((128, 512), jnp.float32)
    for z in range(NZ):
        for copy in copies[z]:
            copy.wait()
        right = jnp.concatenate([w_ref[z, r] for r in range(NY)], axis=1)
        total = total + jnp.dot(a_ref[z], right, preferred_element_type=jnp.float32)
    resid = resid_ref[...].astype(jnp.float32)
    for cc in range(NC):
        for xx in range(NX):
            rows = total[(cc * NX + xx) * 16 : (cc * NX + xx + 1) * 16]
            mine = jnp.logical_and(x == xx, c == cc)
            rows = (rows + jnp.where(mine, resid, 0.0)).astype(jnp.bfloat16)
            for r in range(NY):
                out_ref[lax.rem(y + r, NY), xx * NC + cc] = rows[:, 128 * r : 128 * (r + 1)]


def ring(array):
    above = shifted(array, "y", -1)
    below = shifted(array, "y", 1)
    return above, below


def local(
    tokens,
    seq_pos,
    state,
    norm_in_gain,
    query_weight,
    key_weight,
    value_weight,
    gate_weight,
    head_gain,
    out_weight,
    norm_mlp_gain,
    hidden_weight,
    down_weight,
):
    y = lax.axis_index("y")
    weights = jnp.concatenate([query_weight, key_weight, value_weight, gate_weight], axis=1)
    weights = (weights.astype(jnp.float32) * norm_in_gain[:, None]).astype(jnp.bfloat16)
    width = weights.shape[1]
    above, below = ring(weights)
    far_a = shifted(below[:, : width // 2], "y", 1)
    far_b = shifted(above[:, width // 2 :], "y", -1)

    rows = jnp.broadcast_to(tokens.reshape(NY, 1, 16, 128), (NY, NX * NC, 16, 128))
    rows = exchanged(rows.reshape(NY * NX * NC, 16, 128), ("y", "x", "c"))
    rows = rows.reshape(NY, 128, 128)
    rows = lax.dynamic_slice_in_dim(jnp.concatenate([rows, rows], axis=0), y, NY, 0)

    scaled = (hidden_weight.astype(jnp.float32) * norm_mlp_gain[:, None]).astype(jnp.bfloat16)
    scaled = scaled.reshape(128, NZ, 2, 128).transpose(1, 2, 0, 3).reshape(NZ, 256, 128)
    z = lax.axis_index("z")
    mixer = [lax.dynamic_index_in_dim(scaled, z, 0, keepdims=False)]
    for s in range(1, NZ):
        block = lax.dynamic_index_in_dim(scaled, (z + s) % NZ, 0, keepdims=False)
        mixer.append(shifted(block, "z", s))
    mixer = jnp.stack(mixer)

    heads_dev = 2
    head_ids = (lax.axis_index(TP) * heads_dev + jnp.arange(heads_dev, dtype=jnp.int32)).astype(
        jnp.float32
    )
    decayed = lax.optimization_barrier(head_decay(head_ids)[None, :, None, None] * state)

    def term(left, right):
        return jnp.dot(left, right, preferred_element_type=jnp.float32)

    near = term(rows[0], weights) + term(rows[3], below) + term(rows[1], above)
    far = jnp.concatenate([term(rows[2], far_a), term(rows[2], far_b)], axis=1)
    rows_f = rows.astype(jnp.float32)
    squares = jnp.sum(rows_f * rows_f, axis=(0, 2))[:, None]
    coarse = squares.astype(jnp.bfloat16)
    fine = (squares - coarse.astype(jnp.float32)).astype(jnp.bfloat16)
    terms = jnp.concatenate([(near + far).astype(jnp.bfloat16), coarse, fine], axis=1)
    sums = summed_on_arrival(terms.reshape(NZ, 16, width + 2), "z")
    total_in = sums[:, width] + sums[:, width + 1]
    factor = lax.rsqrt(total_in / D + EPS)[:, None]
    wq, wv = (query_weight.shape[1], value_weight.shape[1])
    query = sums[:, :wq] * factor
    keys = sums[:, wq : 2 * wq] * factor
    values = sums[:, 2 * wq : 2 * wq + wv] * factor
    gates = sums[:, 2 * wq + wv : width] * factor

    mix_above, mix_below = ring(mixer)
    down_above, down_below = ring(down_weight)
    out_above, out_below = ring(out_weight)
    out_far = shifted(out_weight, "y", 2)
    out_wide = jnp.concatenate([out_weight, out_above, out_far, out_below], axis=1)
    out_wide = lax.optimization_barrier(out_wide)

    local_rows = query.shape[0]
    turned_query = rotate(query.reshape(local_rows, heads_dev, DK), seq_pos)
    turned_keys = rotate(keys.reshape(local_rows, heads_dev, DK), seq_pos) * DK ** (-0.5)
    new_state = decayed + jnp.einsum(
        "bhk,bhv->bhkv",
        turned_keys,
        values.reshape(local_rows, heads_dev, DV),
        precision=lax.Precision.HIGHEST,
    )
    read = jnp.einsum("bhk,bhkv->bhv", turned_query, new_state, precision=lax.Precision.HIGHEST)
    read = read * lax.rsqrt(jnp.mean(read * read, axis=-1, keepdims=True) + EPS)
    mixed = (
        read.reshape(local_rows, heads_dev * DV) * head_gain[None, :] * jax.nn.silu(gates)
    ).astype(jnp.bfloat16)
    mixed_all = copy_for_each(mixed, "z").reshape(128, heads_dev * DV)
    attn_terms = term(mixed_all, out_wide).astype(jnp.bfloat16)
    attn = summed_on_arrival(attn_terms.reshape(NX * NC, 16, 512), TP)
    mine = rows.reshape(NY, NX * NC, 16, 128)
    mine = lax.dynamic_index_in_dim(mine, lax.axis_index(TP), 1, keepdims=False)
    mine = mine.transpose(1, 0, 2).reshape(16, 512)
    resid = (mine.astype(jnp.float32) + attn).astype(jnp.bfloat16)

    far_low = shifted(mix_below[: NZ // 2], "y", 1)
    far_high = shifted(mix_above[NZ // 2 :], "y", -1)

    down_low = shifted(down_below[:1024], "y", 1)
    down_high = shifted(down_above[1024:], "y", -1)

    own = copy_for_each(resid, ZX).reshape(NZ, 64, 512)
    other = swapped(own)
    anywhere = pl.BlockSpec(memory_space=pl.ANY)
    active = pl.pallas_call(
        hidden_kernel,
        out_shape=jax.ShapeDtypeStruct((NZ, 128, 256), jnp.bfloat16),
        in_specs=[anywhere] * 7,
        scratch_shapes=[
            pltpu.VMEM((NZ, NC, 64, 512), jnp.bfloat16),
            pltpu.VMEM((NZ, NY, 256, 128), jnp.bfloat16),
            pltpu.SemaphoreType.DMA((NZ, 2)),
            pltpu.SemaphoreType.DMA((NZ, NY)),
        ],
        name="hidden",
    )(own, other, mixer, mix_above, far_low, far_high, mix_below)
    active = exchanged(active, "z")
    partial = pl.pallas_call(
        down_kernel,
        out_shape=jax.ShapeDtypeStruct((NY, NX * NC, 16, 128), jnp.bfloat16),
        in_specs=[anywhere, pl.BlockSpec(memory_space=pltpu.VMEM)] + [anywhere] * 5,
        scratch_shapes=[
            pltpu.VMEM((NZ, 128, 256), jnp.bfloat16),
            pltpu.VMEM((NZ, NY, 256, 128), jnp.bfloat16),
            pltpu.SemaphoreType.DMA((NZ,)),
            pltpu.SemaphoreType.DMA((NZ, NY)),
        ],
        name="down",
    )(active, resid, down_weight, down_above, down_low, down_high, down_below)
    partial = exchanged(partial.reshape(NY * NX * NC, 16, 128), ("y", "x", "c"))
    output = jnp.sum(partial.reshape(NY, NX * NC, 16, 128).astype(jnp.float32), axis=1)
    output = output.astype(jnp.bfloat16).reshape(64, 128)
    return (output, new_state)


def solution(mesh):
    torus = Mesh(mesh.devices.reshape(NZ, NY, NX, NC), ("z", "y", "x", "c"))
    return jax.shard_map(
        local,
        mesh=torus,
        in_specs=(
            P(TP, KV),
            P(KV),
            P(KV, TP, None, None),
            P(KV),
            P(KV, TP),
            P(KV, TP),
            P(KV, TP),
            P(KV, TP),
            P(TP),
            P(TP, KV),
            P(KV),
            P(KV, TP),
            P(TP, KV),
        ),
        out_specs=(P(TP, KV), P(KV, TP, None, None)),
        check_vma=False,
    )
```

```python
import jax
import jax.numpy as jnp
from jax import lax
from jax.experimental import pallas as pl
from jax.experimental.pallas import tpu as pltpu
from jax.sharding import Mesh
from jax.sharding import PartitionSpec as P

D = 4096
H = 16
DK = 128
DV = 256
KV = ("z", "y")
TP = ("x", "c")
ZX = ("z", "x")
NZ, NY, NX, NC = (8, 4, 4, 2)


EPS = 1e-06


def exchanged(blocks, axis):
    return lax.all_to_all(blocks, axis, split_axis=0, concat_axis=0, tiled=True)


def copy_for_each(array, axis):
    copies = jnp.broadcast_to(array, (lax.axis_size(axis), *array.shape))
    return exchanged(copies, axis)


def summed_on_arrival(blocks, axis):
    return jnp.sum(exchanged(blocks, axis).astype(jnp.float32), axis=0)


def shifted(array, axis, by):
    size = lax.axis_size(axis)
    return lax.ppermute(array, axis, [(i, (i + by) % size) for i in range(size)])


def swapped(array):
    return lax.ppermute(array, "c", [(0, 1), (1, 0)])


def rotate(vectors, positions):
    half = vectors.shape[-1] // 2
    inverse = jnp.power(10000.0, -jnp.arange(half, dtype=jnp.float32) / half)
    angles = positions.astype(jnp.float32)[:, None] * inverse[None, :]
    cosine = jnp.cos(angles)[:, None, :]
    sine = jnp.sin(angles)[:, None, :]
    first, second = (vectors[..., :half], vectors[..., half:])
    return jnp.concatenate(
        [first * cosine - second * sine, first * sine + second * cosine], axis=-1
    )


def head_decay(head_ids):
    return 1.0 - jnp.exp2(-2.0 - 6.0 * head_ids / (H - 1))


def far_block(low_ref, high_ref, z, size):
    half = NZ // 2
    ref, at = (low_ref, z) if z < half else (high_ref, z - half)
    return ref.at[pl.ds(at * size, size)]


def hidden_kernel(own_ref, other_ref, w0_ref, w1_ref, w2a_ref, w2b_ref, w3_ref, out_ref, x_ref, w_ref, x_sem, w_sem):
    me = lax.axis_index("c")
    copies = []
    for z in range(NZ):
        parts = [
            pltpu.make_async_copy(own_ref.at[z], x_ref.at[z, me], x_sem.at[z, 0]),
            pltpu.make_async_copy(other_ref.at[z], x_ref.at[z, 1 - me], x_sem.at[z, 1]),
        ]
        far = w2a_ref.at[z] if z < NZ // 2 else w2b_ref.at[z - NZ // 2]
        for r, ref in enumerate([w0_ref.at[z], w1_ref.at[z], far, w3_ref.at[z]]):
            parts.append(pltpu.make_async_copy(ref, w_ref.at[z, r], w_sem.at[z, r]))
        for copy in parts:
            copy.start()
        copies.append(parts)
    rows = own_ref.shape[1]
    hidden = jnp.zeros((2 * rows, 256), jnp.float32)
    squares = jnp.zeros((2 * rows, 1), jnp.float32)
    for z in range(NZ):
        for copy in copies[z]:
            copy.wait()
        left = x_ref[z].reshape(2 * rows, 512)
        wide = left.astype(jnp.float32)
        squares = squares + jnp.sum(wide * wide, axis=1, keepdims=True)
        right = [w_ref[z, :, 128 * j : 128 * (j + 1), :].reshape(512, 128) for j in range(2)]
        right = jnp.concatenate(right, axis=1)
        hidden = hidden + jnp.dot(left, right, preferred_element_type=jnp.float32)
    scale = lax.rsqrt(squares / D + EPS)
    positive = jnp.maximum(hidden * scale, 0.0)
    active = (positive * positive).astype(jnp.bfloat16)
    for z in range(NZ):
        out_ref[z] = active


def down_kernel(act_ref, resid_ref, w0_ref, w1_ref, w2a_ref, w2b_ref, w3_ref, out_ref, a_ref, w_ref, a_sem, w_sem):
    y, x, c = (lax.axis_index("y"), lax.axis_index("x"), lax.axis_index("c"))
    copies = []
    for z in range(NZ):
        parts = [pltpu.make_async_copy(act_ref.at[z], a_ref.at[z], a_sem.at[z])]
        near = [ref.at[pl.ds(256 * z, 256)] for ref in (w0_ref, w1_ref, w3_ref)]
        blocks = [near[0], near[1], far_block(w2a_ref, w2b_ref, z, 256), near[2]]
        for r, ref in enumerate(blocks):
            parts.append(pltpu.make_async_copy(ref, w_ref.at[z, r], w_sem.at[z, r]))
        for copy in parts:
            copy.start()
        copies.append(parts)
    total = jnp.zeros((128, 512), jnp.float32)
    for z in range(NZ):
        for copy in copies[z]:
            copy.wait()
        right = jnp.concatenate([w_ref[z, r] for r in range(NY)], axis=1)
        total = total + jnp.dot(a_ref[z], right, preferred_element_type=jnp.float32)
    resid = resid_ref[...].astype(jnp.float32)
    for cc in range(NC):
        for xx in range(NX):
            rows = total[(cc * NX + xx) * 16 : (cc * NX + xx + 1) * 16]
            mine = jnp.logical_and(x == xx, c == cc)
            rows = (rows + jnp.where(mine, resid, 0.0)).astype(jnp.bfloat16)
            for r in range(NY):
                out_ref[lax.rem(y + r, NY), xx * NC + cc] = rows[:, 128 * r : 128 * (r + 1)]


def ring(array):
    above = shifted(array, "y", -1)
    below = shifted(array, "y", 1)
    return above, below


def local(
    tokens,
    seq_pos,
    state,
    norm_in_gain,
    query_weight,
    key_weight,
    value_weight,
    gate_weight,
    head_gain,
    out_weight,
    norm_mlp_gain,
    hidden_weight,
    down_weight,
):
    y = lax.axis_index("y")
    weights = jnp.concatenate([query_weight, key_weight, value_weight, gate_weight], axis=1)
    weights = (weights.astype(jnp.float32) * norm_in_gain[:, None]).astype(jnp.bfloat16)
    width = weights.shape[1]
    above, below = ring(weights)
    far_a = shifted(below[:, : width // 2], "y", 1)
    far_b = shifted(above[:, width // 2 :], "y", -1)

    rows = jnp.broadcast_to(tokens.reshape(NY, 1, 16, 128), (NY, NX * NC, 16, 128))
    rows = exchanged(rows.reshape(NY * NX * NC, 16, 128), ("y", "x", "c"))
    rows = rows.reshape(NY, 128, 128)
    rows = lax.dynamic_slice_in_dim(jnp.concatenate([rows, rows], axis=0), y, NY, 0)

    scaled = (hidden_weight.astype(jnp.float32) * norm_mlp_gain[:, None]).astype(jnp.bfloat16)
    scaled = scaled.reshape(128, NZ, 2, 128).transpose(1, 2, 0, 3).reshape(NZ, 256, 128)
    mixer = exchanged(scaled, "z")

    def term(left, right):
        return jnp.dot(left, right, preferred_element_type=jnp.float32)

    near = term(rows[0], weights) + term(rows[3], below) + term(rows[1], above)
    far = jnp.concatenate([term(rows[2], far_a), term(rows[2], far_b)], axis=1)
    rows_f = rows.astype(jnp.float32)
    squares = jnp.sum(rows_f * rows_f, axis=(0, 2))[:, None]
    coarse = squares.astype(jnp.bfloat16)
    fine = (squares - coarse.astype(jnp.float32)).astype(jnp.bfloat16)
    terms = jnp.concatenate([(near + far).astype(jnp.bfloat16), coarse, fine], axis=1)
    sums = summed_on_arrival(terms.reshape(NZ, 16, width + 2), "z")
    total_in = sums[:, width] + sums[:, width + 1]
    factor = lax.rsqrt(total_in / D + EPS)[:, None]
    wq, wv = (query_weight.shape[1], value_weight.shape[1])
    query = sums[:, :wq] * factor
    keys = sums[:, wq : 2 * wq] * factor
    values = sums[:, 2 * wq : 2 * wq + wv] * factor
    gates = sums[:, 2 * wq + wv : width] * factor

    mix_above, mix_below = ring(mixer)
    down_above, down_below = ring(down_weight)
    out_above, out_below = ring(out_weight)
    out_far = shifted(out_weight, "y", 2)
    out_wide = jnp.concatenate([out_weight, out_above, out_far, out_below], axis=1)
    out_wide = lax.optimization_barrier(out_wide)

    local_rows = query.shape[0]
    heads_dev = 2
    turned_query = rotate(query.reshape(local_rows, heads_dev, DK), seq_pos)
    turned_keys = rotate(keys.reshape(local_rows, heads_dev, DK), seq_pos) * DK ** (-0.5)
    head_ids = (lax.axis_index(TP) * heads_dev + jnp.arange(heads_dev, dtype=jnp.int32)).astype(
        jnp.float32
    )
    decay = head_decay(head_ids)[None, :, None]
    values = values.reshape(local_rows, heads_dev, DV)
    along = jnp.sum(turned_query * turned_keys, axis=-1, keepdims=True)
    read = decay * jnp.sum(turned_query[..., None] * state, axis=2) + along * values
    read = read * lax.rsqrt(jnp.mean(read * read, axis=-1, keepdims=True) + EPS)
    mixed = (
        read.reshape(local_rows, heads_dev * DV) * head_gain[None, :] * jax.nn.silu(gates)
    ).astype(jnp.bfloat16)
    mixed, old, left, right = lax.optimization_barrier((mixed, state, turned_keys, values))
    new_state = decay[..., None] * old + left[..., None] * right[:, :, None, :]
    mixed_all = copy_for_each(mixed, "z").reshape(128, heads_dev * DV)
    attn_terms = term(mixed_all, out_wide).astype(jnp.bfloat16)
    attn = summed_on_arrival(attn_terms.reshape(NX * NC, 16, 512), TP)
    mine = rows.reshape(NY, NX * NC, 16, 128)
    mine = lax.dynamic_index_in_dim(mine, lax.axis_index(TP), 1, keepdims=False)
    mine = mine.transpose(1, 0, 2).reshape(16, 512)
    resid = (mine.astype(jnp.float32) + attn).astype(jnp.bfloat16)

    far_low = shifted(mix_below[: NZ // 2], "y", 1)
    far_high = shifted(mix_above[NZ // 2 :], "y", -1)

    down_low = shifted(down_below[:1024], "y", 1)
    down_high = shifted(down_above[1024:], "y", -1)

    own = copy_for_each(resid, ZX).reshape(NZ, 64, 512)
    other = swapped(own)
    anywhere = pl.BlockSpec(memory_space=pl.ANY)
    active = pl.pallas_call(
        hidden_kernel,
        out_shape=jax.ShapeDtypeStruct((NZ, 128, 256), jnp.bfloat16),
        in_specs=[anywhere] * 7,
        scratch_shapes=[
            pltpu.VMEM((NZ, NC, 64, 512), jnp.bfloat16),
            pltpu.VMEM((NZ, NY, 256, 128), jnp.bfloat16),
            pltpu.SemaphoreType.DMA((NZ, 2)),
            pltpu.SemaphoreType.DMA((NZ, NY)),
        ],
        name="hidden",
    )(own, other, mixer, mix_above, far_low, far_high, mix_below)
    active = exchanged(active, "z")
    partial = pl.pallas_call(
        down_kernel,
        out_shape=jax.ShapeDtypeStruct((NY, NX * NC, 16, 128), jnp.bfloat16),
        in_specs=[anywhere, pl.BlockSpec(memory_space=pltpu.VMEM)] + [anywhere] * 5,
        scratch_shapes=[
            pltpu.VMEM((NZ, 128, 256), jnp.bfloat16),
            pltpu.VMEM((NZ, NY, 256, 128), jnp.bfloat16),
            pltpu.SemaphoreType.DMA((NZ,)),
            pltpu.SemaphoreType.DMA((NZ, NY)),
        ],
        name="down",
    )(active, resid, down_weight, down_above, down_low, down_high, down_below)
    partial = exchanged(partial.reshape(NY * NX * NC, 16, 128), ("y", "x", "c"))
    output = jnp.sum(partial.reshape(NY, NX * NC, 16, 128).astype(jnp.float32), axis=1)
    output = output.astype(jnp.bfloat16).reshape(64, 128)
    return (output, new_state)


def solution(mesh):
    torus = Mesh(mesh.devices.reshape(NZ, NY, NX, NC), ("z", "y", "x", "c"))
    return jax.shard_map(
        local,
        mesh=torus,
        in_specs=(
            P(TP, KV),
            P(KV),
            P(KV, TP, None, None),
            P(KV),
            P(KV, TP),
            P(KV, TP),
            P(KV, TP),
            P(KV, TP),
            P(TP),
            P(TP, KV),
            P(KV),
            P(KV, TP),
            P(TP, KV),
        ),
        out_specs=(P(TP, KV), P(KV, TP, None, None)),
        check_vma=False,
    )
```

```python
import jax
import jax.numpy as jnp
from jax import lax
from jax.experimental import pallas as pl
from jax.experimental.pallas import tpu as pltpu
from jax.sharding import Mesh
from jax.sharding import PartitionSpec as P

D = 4096
H = 16
DK = 128
DV = 256
KV = ("z", "y")
TP = ("x", "c")
ZX = ("z", "x")
NZ, NY, NX, NC = (8, 4, 4, 2)


EPS = 1e-06


def exchanged(blocks, axis):
    return lax.all_to_all(blocks, axis, split_axis=0, concat_axis=0, tiled=True)


def copy_for_each(array, axis):
    copies = jnp.broadcast_to(array, (lax.axis_size(axis), *array.shape))
    return exchanged(copies, axis)


def summed_on_arrival(blocks, axis):
    return jnp.sum(exchanged(blocks, axis).astype(jnp.float32), axis=0)


def shifted(array, axis, by):
    size = lax.axis_size(axis)
    return lax.ppermute(array, axis, [(i, (i + by) % size) for i in range(size)])


def swapped(array):
    return lax.ppermute(array, "c", [(0, 1), (1, 0)])


def rotate(vectors, positions):
    half = vectors.shape[-1] // 2
    inverse = jnp.power(10000.0, -jnp.arange(half, dtype=jnp.float32) / half)
    angles = positions.astype(jnp.float32)[:, None] * inverse[None, :]
    cosine = jnp.cos(angles)[:, None, :]
    sine = jnp.sin(angles)[:, None, :]
    first, second = (vectors[..., :half], vectors[..., half:])
    return jnp.concatenate(
        [first * cosine - second * sine, first * sine + second * cosine], axis=-1
    )


def head_decay(head_ids):
    return 1.0 - jnp.exp2(-2.0 - 6.0 * head_ids / (H - 1))


STEP = 2


def hidden_kernel(own_ref, other_ref, w0_ref, w1_ref, w2a_ref, w2b_ref, w3_ref, out_ref, x_ref, w_ref, x_sem, w_sem):
    me = lax.axis_index("c")
    copies = []
    for k in range(NZ // STEP):
        at = pl.ds(STEP * k, STEP)
        parts = [
            pltpu.make_async_copy(own_ref.at[at], x_ref.at[me, at], x_sem.at[k, 0]),
            pltpu.make_async_copy(other_ref.at[at], x_ref.at[1 - me, at], x_sem.at[k, 1]),
        ]
        half = NZ // STEP // 2
        far = w2a_ref.at[at] if k < half else w2b_ref.at[pl.ds(STEP * (k - half), STEP)]
        for r, ref in enumerate([w0_ref.at[at], w1_ref.at[at], far, w3_ref.at[at]]):
            parts.append(pltpu.make_async_copy(ref, w_ref.at[r, at], w_sem.at[k, r]))
        for copy in parts:
            copy.start()
        copies.append(parts)
    rows = own_ref.shape[1]
    hidden = jnp.zeros((2 * rows, 256), jnp.float32)
    squares = jnp.zeros((2 * rows, 1), jnp.float32)
    for z in range(NZ):
        if z % STEP == 0:
            for copy in copies[z // STEP]:
                copy.wait()
        left = x_ref[:, z].reshape(2 * rows, 512)
        wide = left.astype(jnp.float32)
        squares = squares + jnp.sum(wide * wide, axis=1, keepdims=True)
        right = [w_ref[:, z, 128 * j : 128 * (j + 1), :].reshape(512, 128) for j in range(2)]
        right = jnp.concatenate(right, axis=1)
        hidden = hidden + jnp.dot(left, right, preferred_element_type=jnp.float32)
    scale = lax.rsqrt(squares / D + EPS)
    positive = jnp.maximum(hidden * scale, 0.0)
    active = (positive * positive).astype(jnp.bfloat16)
    for z in range(NZ):
        out_ref[z] = active


def down_kernel(act_ref, resid_ref, w0_ref, w1_ref, w2a_ref, w2b_ref, w3_ref, out_ref, a_ref, w_ref, a_sem, w_sem):
    y, x, c = (lax.axis_index("y"), lax.axis_index("x"), lax.axis_index("c"))
    copies = []
    size = 256 * STEP
    for k in range(NZ // STEP):
        at = pl.ds(STEP * k, STEP)
        parts = [pltpu.make_async_copy(act_ref.at[at], a_ref.at[at], a_sem.at[k])]
        half = NZ // STEP // 2
        lines = pl.ds(size * k, size)
        far = w2a_ref.at[lines] if k < half else w2b_ref.at[pl.ds(size * (k - half), size)]
        for r, ref in enumerate([w0_ref.at[lines], w1_ref.at[lines], far, w3_ref.at[lines]]):
            parts.append(pltpu.make_async_copy(ref, w_ref.at[r, lines], w_sem.at[k, r]))
        for copy in parts:
            copy.start()
        copies.append(parts)
    total = jnp.zeros((128, 512), jnp.float32)
    for z in range(NZ):
        if z % STEP == 0:
            for copy in copies[z // STEP]:
                copy.wait()
        right = [w_ref[r, 256 * z : 256 * (z + 1)] for r in range(NY)]
        right = jnp.concatenate(right, axis=1)
        total = total + jnp.dot(a_ref[z], right, preferred_element_type=jnp.float32)
    resid = resid_ref[...].astype(jnp.float32)
    for cc in range(NC):
        for xx in range(NX):
            rows = total[(cc * NX + xx) * 16 : (cc * NX + xx + 1) * 16]
            mine = jnp.logical_and(x == xx, c == cc)
            rows = (rows + jnp.where(mine, resid, 0.0)).astype(jnp.bfloat16)
            for r in range(NY):
                out_ref[lax.rem(y + r, NY), xx * NC + cc] = rows[:, 128 * r : 128 * (r + 1)]


def ring(array):
    above = shifted(array, "y", -1)
    below = shifted(array, "y", 1)
    return above, below


def local(
    tokens,
    seq_pos,
    state,
    norm_in_gain,
    query_weight,
    key_weight,
    value_weight,
    gate_weight,
    head_gain,
    out_weight,
    norm_mlp_gain,
    hidden_weight,
    down_weight,
):
    y = lax.axis_index("y")
    weights = jnp.concatenate([query_weight, key_weight, value_weight, gate_weight], axis=1)
    weights = (weights.astype(jnp.float32) * norm_in_gain[:, None]).astype(jnp.bfloat16)
    width = weights.shape[1]
    above, below = ring(weights)
    far_a = shifted(below[:, : width // 2], "y", 1)
    far_b = shifted(above[:, width // 2 :], "y", -1)

    rows = jnp.broadcast_to(tokens.reshape(NY, 1, 16, 128), (NY, NX * NC, 16, 128))
    rows = exchanged(rows.reshape(NY * NX * NC, 16, 128), ("y", "x", "c"))
    rows = rows.reshape(NY, 128, 128)
    rows = lax.dynamic_slice_in_dim(jnp.concatenate([rows, rows], axis=0), y, NY, 0)

    scaled = (hidden_weight.astype(jnp.float32) * norm_mlp_gain[:, None]).astype(jnp.bfloat16)
    scaled = scaled.reshape(128, NZ, 2, 128).transpose(1, 2, 0, 3).reshape(NZ, 256, 128)
    mixer = exchanged(scaled, "z")

    def term(left, right):
        return jnp.dot(left, right, preferred_element_type=jnp.float32)

    near = term(rows[0], weights) + term(rows[3], below) + term(rows[1], above)
    far = jnp.concatenate([term(rows[2], far_a), term(rows[2], far_b)], axis=1)
    rows_f = rows.astype(jnp.float32)
    squares = jnp.sum(rows_f * rows_f, axis=(0, 2))[:, None]
    coarse = squares.astype(jnp.bfloat16)
    fine = (squares - coarse.astype(jnp.float32)).astype(jnp.bfloat16)
    terms = jnp.concatenate([(near + far).astype(jnp.bfloat16), coarse, fine], axis=1)
    sums = summed_on_arrival(terms.reshape(NZ, 16, width + 2), "z")
    total_in = sums[:, width] + sums[:, width + 1]
    factor = lax.rsqrt(total_in / D + EPS)[:, None]
    wq, wv = (query_weight.shape[1], value_weight.shape[1])
    query = sums[:, :wq] * factor
    keys = sums[:, wq : 2 * wq] * factor
    values = sums[:, 2 * wq : 2 * wq + wv] * factor
    gates = sums[:, 2 * wq + wv : width] * factor

    mix_above, mix_below = ring(mixer)
    down_above, down_below = ring(down_weight)
    out_above, out_below = ring(out_weight)
    out_far = shifted(out_weight, "y", 2)
    out_wide = jnp.concatenate([out_weight, out_above, out_far, out_below], axis=1)
    out_wide = lax.optimization_barrier(out_wide)

    local_rows = query.shape[0]
    heads_dev = 2
    turned_query = rotate(query.reshape(local_rows, heads_dev, DK), seq_pos)
    turned_keys = rotate(keys.reshape(local_rows, heads_dev, DK), seq_pos) * DK ** (-0.5)
    head_ids = (lax.axis_index(TP) * heads_dev + jnp.arange(heads_dev, dtype=jnp.int32)).astype(
        jnp.float32
    )
    decay = head_decay(head_ids)[None, :, None]
    values = values.reshape(local_rows, heads_dev, DV)
    along = jnp.sum(turned_query * turned_keys, axis=-1, keepdims=True)
    read = decay * jnp.sum(turned_query[..., None] * state, axis=2) + along * values
    read = read * lax.rsqrt(jnp.mean(read * read, axis=-1, keepdims=True) + EPS)
    mixed = (
        read.reshape(local_rows, heads_dev * DV) * head_gain[None, :] * jax.nn.silu(gates)
    ).astype(jnp.bfloat16)
    mixed, old, left, right = lax.optimization_barrier((mixed, state, turned_keys, values))
    new_state = decay[..., None] * old + left[..., None] * right[:, :, None, :]
    mixed_all = copy_for_each(mixed, "z").reshape(128, heads_dev * DV)
    attn_terms = term(mixed_all, out_wide).astype(jnp.bfloat16)
    attn = summed_on_arrival(attn_terms.reshape(NX * NC, 16, 512), TP)
    mine = rows.reshape(NY, NX * NC, 16, 128)
    mine = lax.dynamic_index_in_dim(mine, lax.axis_index(TP), 1, keepdims=False)
    mine = mine.transpose(1, 0, 2).reshape(16, 512)
    resid = (mine.astype(jnp.float32) + attn).astype(jnp.bfloat16)

    far_low = shifted(mix_below[: NZ // 2], "y", 1)
    far_high = shifted(mix_above[NZ // 2 :], "y", -1)

    down_low = shifted(down_below[:1024], "y", 1)
    down_high = shifted(down_above[1024:], "y", -1)

    own = copy_for_each(resid, ZX).reshape(NZ, 64, 512)
    other = swapped(own)
    anywhere = pl.BlockSpec(memory_space=pl.ANY)
    active = pl.pallas_call(
        hidden_kernel,
        out_shape=jax.ShapeDtypeStruct((NZ, 128, 256), jnp.bfloat16),
        in_specs=[anywhere] * 7,
        scratch_shapes=[
            pltpu.VMEM((NC, NZ, 64, 512), jnp.bfloat16),
            pltpu.VMEM((NY, NZ, 256, 128), jnp.bfloat16),
            pltpu.SemaphoreType.DMA((NZ // STEP, 2)),
            pltpu.SemaphoreType.DMA((NZ // STEP, NY)),
        ],
        name="hidden",
    )(own, other, mixer, mix_above, far_low, far_high, mix_below)
    active = exchanged(active, "z")
    partial = pl.pallas_call(
        down_kernel,
        out_shape=jax.ShapeDtypeStruct((NY, NX * NC, 16, 128), jnp.bfloat16),
        in_specs=[anywhere, pl.BlockSpec(memory_space=pltpu.VMEM)] + [anywhere] * 5,
        scratch_shapes=[
            pltpu.VMEM((NZ, 128, 256), jnp.bfloat16),
            pltpu.VMEM((NY, NZ * 256, 128), jnp.bfloat16),
            pltpu.SemaphoreType.DMA((NZ // STEP,)),
            pltpu.SemaphoreType.DMA((NZ // STEP, NY)),
        ],
        name="down",
    )(active, resid, down_weight, down_above, down_low, down_high, down_below)
    partial = exchanged(partial.reshape(NY * NX * NC, 16, 128), ("y", "x", "c"))
    output = jnp.sum(partial.reshape(NY, NX * NC, 16, 128).astype(jnp.float32), axis=1)
    output = output.astype(jnp.bfloat16).reshape(64, 128)
    return (output, new_state)


def solution(mesh):
    torus = Mesh(mesh.devices.reshape(NZ, NY, NX, NC), ("z", "y", "x", "c"))
    return jax.shard_map(
        local,
        mesh=torus,
        in_specs=(
            P(TP, KV),
            P(KV),
            P(KV, TP, None, None),
            P(KV),
            P(KV, TP),
            P(KV, TP),
            P(KV, TP),
            P(KV, TP),
            P(TP),
            P(TP, KV),
            P(KV),
            P(KV, TP),
            P(TP, KV),
        ),
        out_specs=(P(TP, KV), P(KV, TP, None, None)),
        check_vma=False,
    )
```

```python
import jax
import jax.numpy as jnp
from jax import lax
from jax.experimental import pallas as pl
from jax.experimental.pallas import tpu as pltpu
from jax.sharding import Mesh
from jax.sharding import PartitionSpec as P

D = 4096
H = 16
DK = 128
DV = 256
KV = ("z", "y")
TP = ("x", "c")
XZ = ("x", "z")
NZ, NY, NX, NC = (8, 4, 4, 2)


EPS = 1e-06


def exchanged(blocks, axis):
    return lax.all_to_all(blocks, axis, split_axis=0, concat_axis=0, tiled=True)


def copy_for_each(array, axis):
    copies = jnp.broadcast_to(array, (lax.axis_size(axis), *array.shape))
    return exchanged(copies, axis)


def summed_on_arrival(blocks, axis):
    return jnp.sum(exchanged(blocks, axis).astype(jnp.float32), axis=0)


def shifted(array, axis, by):
    size = lax.axis_size(axis)
    return lax.ppermute(array, axis, [(i, (i + by) % size) for i in range(size)])


def swapped(array):
    return lax.ppermute(array, "c", [(0, 1), (1, 0)])


def rotate(vectors, positions):
    half = vectors.shape[-1] // 2
    inverse = jnp.power(10000.0, -jnp.arange(half, dtype=jnp.float32) / half)
    angles = positions.astype(jnp.float32)[:, None] * inverse[None, :]
    cosine = jnp.cos(angles)[:, None, :]
    sine = jnp.sin(angles)[:, None, :]
    first, second = (vectors[..., :half], vectors[..., half:])
    return jnp.concatenate(
        [first * cosine - second * sine, first * sine + second * cosine], axis=-1
    )


def head_decay(head_ids):
    return 1.0 - jnp.exp2(-2.0 - 6.0 * head_ids / (H - 1))


STEP = 2


def hidden_kernel(own_ref, other_ref, w0_ref, w1_ref, w2a_ref, w2b_ref, w3_ref, out_ref, x_ref, w_ref, x_sem, w_sem):
    me = lax.axis_index("c")
    copies = []
    for k in range(NZ // STEP):
        at = pl.ds(STEP * k, STEP)
        parts = [
            pltpu.make_async_copy(own_ref.at[:, at], x_ref.at[me, :, at], x_sem.at[k, 0]),
            pltpu.make_async_copy(other_ref.at[:, at], x_ref.at[1 - me, :, at], x_sem.at[k, 1]),
        ]
        half = NZ // STEP // 2
        far = w2a_ref.at[at] if k < half else w2b_ref.at[pl.ds(STEP * (k - half), STEP)]
        for r, ref in enumerate([w0_ref.at[at], w1_ref.at[at], far, w3_ref.at[at]]):
            parts.append(pltpu.make_async_copy(ref, w_ref.at[r, at], w_sem.at[k, r]))
        for copy in parts:
            copy.start()
        copies.append(parts)
    hidden = jnp.zeros((128, 256), jnp.float32)
    squares = jnp.zeros((128, 128), jnp.float32)
    for z in range(NZ):
        if z % STEP == 0:
            for copy in copies[z // STEP]:
                copy.wait()
        left = x_ref[:, :, z].reshape(128, 512)
        wide = left.astype(jnp.float32)
        wide = wide * wide
        for j in range(4):
            squares = squares + wide[:, 128 * j : 128 * (j + 1)]
        right = [w_ref[:, z, 128 * j : 128 * (j + 1), :].reshape(512, 128) for j in range(2)]
        right = jnp.concatenate(right, axis=1)
        hidden = hidden + jnp.dot(left, right, preferred_element_type=jnp.float32)
    scale = lax.rsqrt(jnp.sum(squares, axis=1, keepdims=True) / D + EPS)
    positive = jnp.maximum(hidden * scale, 0.0)
    active = (positive * positive).astype(jnp.bfloat16)
    for z in range(NZ):
        out_ref[z] = active


def down_kernel(act_ref, resid_ref, w0_ref, w1_ref, w2a_ref, w2b_ref, w3_ref, out_ref, a_ref, w_ref, a_sem, w_sem):
    y, x, c = (lax.axis_index("y"), lax.axis_index("x"), lax.axis_index("c"))
    copies = []
    size = 256 * STEP
    for k in range(NZ // STEP):
        at = pl.ds(STEP * k, STEP)
        parts = [pltpu.make_async_copy(act_ref.at[at], a_ref.at[at], a_sem.at[k])]
        half = NZ // STEP // 2
        lines = pl.ds(size * k, size)
        far = w2a_ref.at[lines] if k < half else w2b_ref.at[pl.ds(size * (k - half), size)]
        for r, ref in enumerate([w0_ref.at[lines], w1_ref.at[lines], far, w3_ref.at[lines]]):
            parts.append(pltpu.make_async_copy(ref, w_ref.at[r, lines], w_sem.at[k, r]))
        for copy in parts:
            copy.start()
        copies.append(parts)
    total = jnp.zeros((128, 512), jnp.float32)
    for z in range(NZ):
        if z % STEP == 0:
            for copy in copies[z // STEP]:
                copy.wait()
        right = [w_ref[r, 256 * z : 256 * (z + 1)] for r in range(NY)]
        right = jnp.concatenate(right, axis=1)
        total = total + jnp.dot(a_ref[z], right, preferred_element_type=jnp.float32)
    resid = resid_ref[...].astype(jnp.float32)
    for cc in range(NC):
        for xx in range(NX):
            rows = total[(cc * NX + xx) * 16 : (cc * NX + xx + 1) * 16]
            mine = jnp.logical_and(x == xx, c == cc)
            rows = (rows + jnp.where(mine, resid, 0.0)).astype(jnp.bfloat16)
            for r in range(NY):
                out_ref[lax.rem(y + r, NY), xx * NC + cc] = rows[:, 128 * r : 128 * (r + 1)]


def ring(array):
    above = shifted(array, "y", -1)
    below = shifted(array, "y", 1)
    return above, below


def local(
    tokens,
    seq_pos,
    state,
    norm_in_gain,
    query_weight,
    key_weight,
    value_weight,
    gate_weight,
    head_gain,
    out_weight,
    norm_mlp_gain,
    hidden_weight,
    down_weight,
):
    y = lax.axis_index("y")
    weights = jnp.concatenate([query_weight, key_weight, value_weight, gate_weight], axis=1)
    weights = (weights.astype(jnp.float32) * norm_in_gain[:, None]).astype(jnp.bfloat16)
    width = weights.shape[1]
    above, below = ring(weights)
    far_a = shifted(below[:, : width // 2], "y", 1)
    far_b = shifted(above[:, width // 2 :], "y", -1)

    rows = jnp.broadcast_to(tokens.reshape(NY, 1, 16, 128), (NY, NX * NC, 16, 128))
    rows = exchanged(rows.reshape(NY * NX * NC, 16, 128), ("y", "x", "c"))
    rows = rows.reshape(NY, 128, 128)
    rows = lax.dynamic_slice_in_dim(jnp.concatenate([rows, rows], axis=0), y, NY, 0)

    scaled = (hidden_weight.astype(jnp.float32) * norm_mlp_gain[:, None]).astype(jnp.bfloat16)
    scaled = scaled.reshape(128, NZ, 2, 128).transpose(1, 2, 0, 3).reshape(NZ, 256, 128)
    mixer = exchanged(scaled, "z")

    def term(left, right):
        return jnp.dot(left, right, preferred_element_type=jnp.float32)

    near = term(rows[0], weights) + term(rows[3], below) + term(rows[1], above)
    far = jnp.concatenate([term(rows[2], far_a), term(rows[2], far_b)], axis=1)
    rows_f = rows.astype(jnp.float32)
    squares = jnp.sum(rows_f * rows_f, axis=(0, 2))[:, None]
    coarse = squares.astype(jnp.bfloat16)
    fine = (squares - coarse.astype(jnp.float32)).astype(jnp.bfloat16)
    terms = jnp.concatenate([(near + far).astype(jnp.bfloat16), coarse, fine], axis=1)
    sums = summed_on_arrival(terms.reshape(NZ, 16, width + 2), "z")
    total_in = sums[:, width] + sums[:, width + 1]
    factor = lax.rsqrt(total_in / D + EPS)[:, None]
    wq, wv = (query_weight.shape[1], value_weight.shape[1])
    query = sums[:, :wq] * factor
    keys = sums[:, wq : 2 * wq] * factor
    values = sums[:, 2 * wq : 2 * wq + wv] * factor
    gates = sums[:, 2 * wq + wv : width] * factor

    mix_above, mix_below = ring(mixer)
    down_above, down_below = ring(down_weight)
    out_above, out_below = ring(out_weight)
    out_far = shifted(out_weight, "y", 2)
    out_wide = jnp.concatenate([out_weight, out_above, out_far, out_below], axis=1)
    out_wide = lax.optimization_barrier(out_wide)

    local_rows = query.shape[0]
    heads_dev = 2
    turned_query = rotate(query.reshape(local_rows, heads_dev, DK), seq_pos)
    turned_keys = rotate(keys.reshape(local_rows, heads_dev, DK), seq_pos) * DK ** (-0.5)
    head_ids = (lax.axis_index(TP) * heads_dev + jnp.arange(heads_dev, dtype=jnp.int32)).astype(
        jnp.float32
    )
    decay = head_decay(head_ids)[None, :, None]
    values = values.reshape(local_rows, heads_dev, DV)
    along = jnp.sum(turned_query * turned_keys, axis=-1, keepdims=True)
    read = decay * jnp.sum(turned_query[..., None] * state, axis=2) + along * values
    read = read * lax.rsqrt(jnp.mean(read * read, axis=-1, keepdims=True) + EPS)
    mixed = (
        read.reshape(local_rows, heads_dev * DV) * head_gain[None, :] * jax.nn.silu(gates)
    ).astype(jnp.bfloat16)
    mixed, old, left, right = lax.optimization_barrier((mixed, state, turned_keys, values))
    new_state = decay[..., None] * old + left[..., None] * right[:, :, None, :]
    mixed_all = copy_for_each(mixed, "z").reshape(128, heads_dev * DV)
    attn_terms = term(mixed_all, out_wide).astype(jnp.bfloat16)
    attn = summed_on_arrival(attn_terms.reshape(NX * NC, 16, 512), TP)
    mine = rows.reshape(NY, NX * NC, 16, 128)
    mine = lax.dynamic_index_in_dim(mine, lax.axis_index(TP), 1, keepdims=False)
    mine = mine.transpose(1, 0, 2).reshape(16, 512)
    resid = (mine.astype(jnp.float32) + attn).astype(jnp.bfloat16)

    far_low = shifted(mix_below[: NZ // 2], "y", 1)
    far_high = shifted(mix_above[NZ // 2 :], "y", -1)

    down_low = shifted(down_below[:1024], "y", 1)
    down_high = shifted(down_above[1024:], "y", -1)

    own = copy_for_each(resid, XZ).reshape(NX, NZ, 16, 512)
    other = swapped(own)
    anywhere = pl.BlockSpec(memory_space=pl.ANY)
    active = pl.pallas_call(
        hidden_kernel,
        out_shape=jax.ShapeDtypeStruct((NZ, 128, 256), jnp.bfloat16),
        in_specs=[anywhere] * 7,
        scratch_shapes=[
            pltpu.VMEM((NC, NX, NZ, 16, 512), jnp.bfloat16),
            pltpu.VMEM((NY, NZ, 256, 128), jnp.bfloat16),
            pltpu.SemaphoreType.DMA((NZ // STEP, 2)),
            pltpu.SemaphoreType.DMA((NZ // STEP, NY)),
        ],
        name="hidden",
    )(own, other, mixer, mix_above, far_low, far_high, mix_below)
    active = exchanged(active, "z")
    partial = pl.pallas_call(
        down_kernel,
        out_shape=jax.ShapeDtypeStruct((NY, NX * NC, 16, 128), jnp.bfloat16),
        in_specs=[anywhere, pl.BlockSpec(memory_space=pltpu.VMEM)] + [anywhere] * 5,
        scratch_shapes=[
            pltpu.VMEM((NZ, 128, 256), jnp.bfloat16),
            pltpu.VMEM((NY, NZ * 256, 128), jnp.bfloat16),
            pltpu.SemaphoreType.DMA((NZ // STEP,)),
            pltpu.SemaphoreType.DMA((NZ // STEP, NY)),
        ],
        name="down",
    )(active, resid, down_weight, down_above, down_low, down_high, down_below)
    partial = exchanged(partial.reshape(NY * NX * NC, 16, 128), ("y", "x", "c"))
    output = jnp.sum(partial.reshape(NY, NX * NC, 16, 128).astype(jnp.float32), axis=1)
    output = output.astype(jnp.bfloat16).reshape(64, 128)
    return (output, new_state)


def solution(mesh):
    torus = Mesh(mesh.devices.reshape(NZ, NY, NX, NC), ("z", "y", "x", "c"))
    return jax.shard_map(
        local,
        mesh=torus,
        in_specs=(
            P(TP, KV),
            P(KV),
            P(KV, TP, None, None),
            P(KV),
            P(KV, TP),
            P(KV, TP),
            P(KV, TP),
            P(KV, TP),
            P(TP),
            P(TP, KV),
            P(KV),
            P(KV, TP),
            P(TP, KV),
        ),
        out_specs=(P(TP, KV), P(KV, TP, None, None)),
        check_vma=False,
    )
```

```python
import jax
import jax.numpy as jnp
from jax import lax
from jax.experimental import pallas as pl
from jax.experimental.pallas import tpu as pltpu
from jax.sharding import Mesh
from jax.sharding import PartitionSpec as P

D = 4096
H = 16
DK = 128
DV = 256
KV = ("z", "y")
TP = ("x", "c")
XZ = ("x", "z")
NZ, NY, NX, NC = (8, 4, 4, 2)


EPS = 1e-06


def exchanged(blocks, axis):
    return lax.all_to_all(blocks, axis, split_axis=0, concat_axis=0, tiled=True)


def copy_for_each(array, axis):
    copies = jnp.broadcast_to(array, (lax.axis_size(axis), *array.shape))
    return exchanged(copies, axis)


def summed_on_arrival(blocks, axis):
    return jnp.sum(exchanged(blocks, axis).astype(jnp.float32), axis=0)


def shifted(array, axis, by):
    size = lax.axis_size(axis)
    return lax.ppermute(array, axis, [(i, (i + by) % size) for i in range(size)])


def swapped(array):
    return lax.ppermute(array, "c", [(0, 1), (1, 0)])


def rotate(vectors, positions):
    half = vectors.shape[-1] // 2
    inverse = jnp.power(10000.0, -jnp.arange(half, dtype=jnp.float32) / half)
    angles = positions.astype(jnp.float32)[:, None] * inverse[None, :]
    cosine = jnp.cos(angles)[:, None, :]
    sine = jnp.sin(angles)[:, None, :]
    first, second = (vectors[..., :half], vectors[..., half:])
    return jnp.concatenate(
        [first * cosine - second * sine, first * sine + second * cosine], axis=-1
    )


def head_decay(head_ids):
    return 1.0 - jnp.exp2(-2.0 - 6.0 * head_ids / (H - 1))


STEP = 4


def hidden_kernel(own_ref, other_ref, w0_ref, w1_ref, w2a_ref, w2b_ref, w3_ref, out_ref, x_ref, w_ref, x_sem, w_sem):
    me = lax.axis_index("c")
    copies = []
    for k in range(NZ // STEP):
        at = pl.ds(STEP * k, STEP)
        parts = [
            pltpu.make_async_copy(own_ref.at[:, at], x_ref.at[me, :, at], x_sem.at[k, 0]),
            pltpu.make_async_copy(other_ref.at[:, at], x_ref.at[1 - me, :, at], x_sem.at[k, 1]),
        ]
        half = NZ // STEP // 2
        far = w2a_ref.at[at] if k < half else w2b_ref.at[pl.ds(STEP * (k - half), STEP)]
        for r, ref in enumerate([w0_ref.at[at], w1_ref.at[at], far, w3_ref.at[at]]):
            parts.append(pltpu.make_async_copy(ref, w_ref.at[r, at], w_sem.at[k, r]))
        for copy in parts:
            copy.start()
        copies.append(parts)
    hidden = jnp.zeros((128, 256), jnp.float32)
    squares = jnp.zeros((128, 128), jnp.float32)
    for z in range(NZ):
        if z % STEP == 0:
            for copy in copies[z // STEP]:
                copy.wait()
        left = x_ref[:, :, z].reshape(128, 512)
        wide = left.astype(jnp.float32)
        wide = wide * wide
        for j in range(4):
            squares = squares + wide[:, 128 * j : 128 * (j + 1)]
        right = [w_ref[:, z, 128 * j : 128 * (j + 1), :].reshape(512, 128) for j in range(2)]
        right = jnp.concatenate(right, axis=1)
        hidden = hidden + jnp.dot(left, right, preferred_element_type=jnp.float32)
    scale = lax.rsqrt(jnp.sum(squares, axis=1, keepdims=True) / D + EPS)
    positive = jnp.maximum(hidden * scale, 0.0)
    active = (positive * positive).astype(jnp.bfloat16)
    out_ref[...] = active


def down_kernel(act_ref, resid_ref, w0_ref, w1_ref, w2a_ref, w2b_ref, w3_ref, out_ref, a_ref, w_ref, a_sem, w_sem):
    y, x, c = (lax.axis_index("y"), lax.axis_index("x"), lax.axis_index("c"))
    copies = []
    size = 256 * STEP
    for k in range(NZ // STEP):
        at = pl.ds(STEP * k, STEP)
        parts = [pltpu.make_async_copy(act_ref.at[at], a_ref.at[at], a_sem.at[k])]
        half = NZ // STEP // 2
        lines = pl.ds(size * k, size)
        far = w2a_ref.at[lines] if k < half else w2b_ref.at[pl.ds(size * (k - half), size)]
        for r, ref in enumerate([w0_ref.at[lines], w1_ref.at[lines], far, w3_ref.at[lines]]):
            parts.append(pltpu.make_async_copy(ref, w_ref.at[r, lines], w_sem.at[k, r]))
        for copy in parts:
            copy.start()
        copies.append(parts)
    total = jnp.zeros((128, 512), jnp.float32)
    for z in range(NZ):
        if z % STEP == 0:
            for copy in copies[z // STEP]:
                copy.wait()
        right = [w_ref[r, 256 * z : 256 * (z + 1)] for r in range(NY)]
        right = jnp.concatenate(right, axis=1)
        total = total + jnp.dot(a_ref[z], right, preferred_element_type=jnp.float32)
    resid = resid_ref[...].astype(jnp.float32)
    for cc in range(NC):
        for xx in range(NX):
            rows = total[(cc * NX + xx) * 16 : (cc * NX + xx + 1) * 16]
            mine = jnp.logical_and(x == xx, c == cc)
            rows = (rows + jnp.where(mine, resid, 0.0)).astype(jnp.bfloat16)
            for r in range(NY):
                out_ref[lax.rem(y + r, NY), xx * NC + cc] = rows[:, 128 * r : 128 * (r + 1)]


def ring(array):
    above = shifted(array, "y", -1)
    below = shifted(array, "y", 1)
    return above, below


def local(
    tokens,
    seq_pos,
    state,
    norm_in_gain,
    query_weight,
    key_weight,
    value_weight,
    gate_weight,
    head_gain,
    out_weight,
    norm_mlp_gain,
    hidden_weight,
    down_weight,
):
    y = lax.axis_index("y")
    weights = jnp.concatenate([query_weight, key_weight, value_weight, gate_weight], axis=1)
    weights = (weights.astype(jnp.float32) * norm_in_gain[:, None]).astype(jnp.bfloat16)
    width = weights.shape[1]
    above, below = ring(weights)
    far_a = shifted(below[:, : width // 2], "y", 1)
    far_b = shifted(above[:, width // 2 :], "y", -1)

    rows = jnp.broadcast_to(tokens.reshape(NY, 1, 16, 128), (NY, NX * NC, 16, 128))
    rows = exchanged(rows.reshape(NY * NX * NC, 16, 128), ("y", "x", "c"))
    rows = rows.reshape(NY, 128, 128)
    rows = lax.dynamic_slice_in_dim(jnp.concatenate([rows, rows], axis=0), y, NY, 0)

    scaled = (hidden_weight.astype(jnp.float32) * norm_mlp_gain[:, None]).astype(jnp.bfloat16)
    scaled = scaled.reshape(128, NZ, 2, 128).transpose(1, 2, 0, 3).reshape(NZ, 256, 128)
    mixer = exchanged(scaled, "z")

    def term(left, right):
        return jnp.dot(left, right, preferred_element_type=jnp.float32)

    near = term(rows[0], weights) + term(rows[3], below) + term(rows[1], above)
    far = jnp.concatenate([term(rows[2], far_a), term(rows[2], far_b)], axis=1)
    rows_f = rows.astype(jnp.float32)
    squares = jnp.sum(rows_f * rows_f, axis=(0, 2))[:, None]
    coarse = squares.astype(jnp.bfloat16)
    fine = (squares - coarse.astype(jnp.float32)).astype(jnp.bfloat16)
    terms = jnp.concatenate([(near + far).astype(jnp.bfloat16), coarse, fine], axis=1)
    sums = summed_on_arrival(terms.reshape(NZ, 16, width + 2), "z")
    total_in = sums[:, width] + sums[:, width + 1]
    factor = lax.rsqrt(total_in / D + EPS)[:, None]
    wq, wv = (query_weight.shape[1], value_weight.shape[1])
    query = sums[:, :wq] * factor
    keys = sums[:, wq : 2 * wq] * factor
    values = sums[:, 2 * wq : 2 * wq + wv] * factor
    gates = sums[:, 2 * wq + wv : width] * factor

    mix_above, mix_below = ring(mixer)
    down_above, down_below = ring(down_weight)
    out_above, out_below = ring(out_weight)
    out_far = shifted(out_weight, "y", 2)
    out_wide = jnp.concatenate([out_weight, out_above, out_far, out_below], axis=1)
    out_wide = lax.optimization_barrier(out_wide)

    local_rows = query.shape[0]
    heads_dev = 2
    turned_query = rotate(query.reshape(local_rows, heads_dev, DK), seq_pos)
    turned_keys = rotate(keys.reshape(local_rows, heads_dev, DK), seq_pos) * DK ** (-0.5)
    head_ids = (lax.axis_index(TP) * heads_dev + jnp.arange(heads_dev, dtype=jnp.int32)).astype(
        jnp.float32
    )
    decay = head_decay(head_ids)[None, :, None]
    values = values.reshape(local_rows, heads_dev, DV)
    along = jnp.sum(turned_query * turned_keys, axis=-1, keepdims=True)
    read = decay * jnp.sum(turned_query[..., None] * state, axis=2) + along * values
    read = read * lax.rsqrt(jnp.mean(read * read, axis=-1, keepdims=True) + EPS)
    mixed = (
        read.reshape(local_rows, heads_dev * DV) * head_gain[None, :] * jax.nn.silu(gates)
    ).astype(jnp.bfloat16)
    mixed_all = copy_for_each(mixed, "z").reshape(128, heads_dev * DV)
    attn_terms = term(mixed_all, out_wide).astype(jnp.bfloat16)
    attn = summed_on_arrival(attn_terms.reshape(NX * NC, 16, 512), TP)
    mine = rows.reshape(NY, NX * NC, 16, 128)
    mine = lax.dynamic_index_in_dim(mine, lax.axis_index(TP), 1, keepdims=False)
    mine = mine.transpose(1, 0, 2).reshape(16, 512)
    resid = (mine.astype(jnp.float32) + attn).astype(jnp.bfloat16)

    far_low = shifted(mix_below[: NZ // 2], "y", 1)
    far_high = shifted(mix_above[NZ // 2 :], "y", -1)

    down_low = shifted(down_below[:1024], "y", 1)
    down_high = shifted(down_above[1024:], "y", -1)

    own = copy_for_each(resid, XZ).reshape(NX, NZ, 16, 512)
    other = swapped(own)
    anywhere = pl.BlockSpec(memory_space=pl.ANY)
    active = pl.pallas_call(
        hidden_kernel,
        out_shape=jax.ShapeDtypeStruct((128, 256), jnp.bfloat16),
        in_specs=[anywhere] * 7,
        scratch_shapes=[
            pltpu.VMEM((NC, NX, NZ, 16, 512), jnp.bfloat16),
            pltpu.VMEM((NY, NZ, 256, 128), jnp.bfloat16),
            pltpu.SemaphoreType.DMA((NZ // STEP, 2)),
            pltpu.SemaphoreType.DMA((NZ // STEP, NY)),
        ],
        name="hidden",
    )(own, other, mixer, mix_above, far_low, far_high, mix_below)
    active, down_low, down_high = lax.optimization_barrier((active, down_low, down_high))
    active = copy_for_each(active, "z").reshape(NZ, 128, 256)
    partial = pl.pallas_call(
        down_kernel,
        out_shape=jax.ShapeDtypeStruct((NY, NX * NC, 16, 128), jnp.bfloat16),
        in_specs=[anywhere, pl.BlockSpec(memory_space=pltpu.VMEM)] + [anywhere] * 5,
        scratch_shapes=[
            pltpu.VMEM((NZ, 128, 256), jnp.bfloat16),
            pltpu.VMEM((NY, NZ * 256, 128), jnp.bfloat16),
            pltpu.SemaphoreType.DMA((NZ // STEP,)),
            pltpu.SemaphoreType.DMA((NZ // STEP, NY)),
        ],
        name="down",
    )(active, resid, down_weight, down_above, down_low, down_high, down_below)
    partial, old, left, right = lax.optimization_barrier((partial, state, turned_keys, values))
    new_state = decay[..., None] * old + left[..., None] * right[:, :, None, :]
    partial = exchanged(partial.reshape(NY * NX * NC, 16, 128), ("y", "x", "c"))
    output = jnp.sum(partial.reshape(NY, NX * NC, 16, 128).astype(jnp.float32), axis=1)
    output = output.astype(jnp.bfloat16).reshape(64, 128)
    return (output, new_state)


def solution(mesh):
    torus = Mesh(mesh.devices.reshape(NZ, NY, NX, NC), ("z", "y", "x", "c"))
    return jax.shard_map(
        local,
        mesh=torus,
        in_specs=(
            P(TP, KV),
            P(KV),
            P(KV, TP, None, None),
            P(KV),
            P(KV, TP),
            P(KV, TP),
            P(KV, TP),
            P(KV, TP),
            P(TP),
            P(TP, KV),
            P(KV),
            P(KV, TP),
            P(TP, KV),
        ),
        out_specs=(P(TP, KV), P(KV, TP, None, None)),
        check_vma=False,
    )
```
